32 devices in a mesh: sp: 8 (over z, core), tp: 4 (over y, x).
Axes of the slice: x: 2, y: 2, z: 4, core: 2. Of those that a mesh axis runs over, the one named last changes fastest.
Arguments:
- cotangent: bfloat16 [1024, 2048], P('sp'), may hold values from -6 to 6
- moe_input: bfloat16 [1024, 2048], P('sp'), may hold values from -6 to 6
- expert_ids: int32 [1024, 2], P('sp'), may hold values from 0 to 7, all different within a row; in each aligned block of 128 rows (0 to 127, 128 to 255, ...) at most 48 rows name the same one
- group_weight: float32 [1024], P('sp'), may hold values from 0.3 to 1
- expert_weight: float32 [1024, 2], P('sp'), may hold values from 0.1 to 0.9
- mixer_out: bfloat16 [1024, 512], P('sp', 'tp'), may hold values from -6 to 6
- queries: bfloat16 [256, 1024], P('tp', 'sp'), may hold values from -6 to 6
- key_vectors: bfloat16 [256, 1024], P('tp', 'sp'), may hold values from -6 to 6
- value_vectors: bfloat16 [512, 1024], P('tp', 'sp'), may hold values from -6 to 6
- decay_rates: float32 [4, 1024], P('tp', 'sp'), may hold values from 0 to 1, as said below
- proj_weight: bfloat16 [2048, 512], P(None, 'tp'), may hold values from -0.25 to 0.25
- gate_weight: bfloat16 [8, 2048, 2048], P('sp', None, 'tp'), may hold values from -0.125 to 0.125
- up_weight: bfloat16 [8, 2048, 2048], P('sp', None, 'tp'), may hold values from -0.125 to 0.125
- down_weight: bfloat16 [8, 2048, 2048], P('sp', 'tp'), may hold values from -0.125 to 0.125
Outputs:
- grad_gate: bfloat16 [8, 2048, 2048], P('sp', None, 'tp')
- grad_up: bfloat16 [8, 2048, 2048], P('sp', None, 'tp')
- grad_down: bfloat16 [8, 2048, 2048], P('sp', 'tp')
- grad_proj: float32 [2048, 512], P('sp', 'tp')
- grad_queries: float32 [256, 1024], P('tp', 'sp')
- grad_keys: float32 [256, 1024], P('tp', 'sp')
- grad_values: float32 [512, 1024], P('tp', 'sp')
The draws below stay inside these ranges and needn't reach their ends.
Inputs may be any that keep to these rules, and one draw needn't show every extreme that they name: `expert_ids`: in the rows of one device no expert is named by more than 48 entries, a bound that some block reaches; the 2 experts of a row differ. `decay_rates`: Positive.
All inputs are finite; a program needn't handle non-finite values.
Results may differ from the reference program's by a relative error of at most 0.0058.
Values may be sent and summed in bfloat16 or wider, within the bound.
A program may use at most 64 MiB of HBM per device.

```python
import math
from functools import partial
import jax
import jax.numpy as jnp
import numpy as np
from jax import lax

D = 2048
KD = 64
VD = 128
RETENTION_HEADS = 4
FF = 2048
EXPERTS = 8
TOP = 2
TOK_DEV = 128
SEQUENCE_TOKENS = 1024
CAP = 48
N_SP = 8


def draw_decay_rates(key, part):
    random_subkeys = jax.random.split(key, 6)
    fast_share = 0.5
    fast_heads = jax.random.uniform(random_subkeys[0], (RETENTION_HEADS, 1)) < fast_share
    block_count = SEQUENCE_TOKENS // TOK_DEV
    block_multiplier = jax.random.uniform(random_subkeys[1], (RETENTION_HEADS, block_count, 1), minval=0.5, maxval=1.5)
    block_multiplier = jnp.broadcast_to(block_multiplier, (RETENTION_HEADS, block_count, TOK_DEV)).reshape(RETENTION_HEADS, SEQUENCE_TOKENS)
    jaggedness = jnp.exp(jax.random.uniform(random_subkeys[2], (RETENTION_HEADS, SEQUENCE_TOKENS), minval=math.log(0.7), maxval=math.log(1.4)))
    fast_rate = jnp.exp(jax.random.uniform(random_subkeys[3], (RETENTION_HEADS, 1), minval=math.log(1.0 / 40.0), maxval=math.log(1.0 / 15.0)))
    baseline_rate = jnp.where(fast_heads, fast_rate, 0.8 / SEQUENCE_TOKENS)
    spike_position = jax.random.randint(random_subkeys[4], (RETENTION_HEADS, 2, 1), 0, SEQUENCE_TOKENS)
    spike_penalty = jax.random.uniform(random_subkeys[5], (RETENTION_HEADS, 2, 1), minval=0.2, maxval=0.4)
    token_positions = jnp.arange(SEQUENCE_TOKENS, dtype=jnp.int32)[None, None, :]
    spike_events = jnp.sum(jnp.where(token_positions == spike_position, -jnp.log(1.0 - spike_penalty), 0.0), axis=1)
    return (baseline_rate * block_multiplier * jaggedness + spike_events).astype(jnp.float32)


def with_spikes(array, rng, source, target, blocks, factor):
    owner, partner = [(jnp.arange(array.shape[dim]) // (array.shape[dim] // blocks)).reshape([-1 if axis == dim else 1 for axis in range(array.ndim)]) for dim in (source, target)]
    chosen = jax.random.permutation(rng, blocks)[partner]
    strong = (owner == chosen) | (owner == (partner + blocks // 2) % blocks)
    return jnp.where(strong, factor * array, array)


def level_of(rng, shape, pieces, low, high):
    def one(dim, blocks):
        heights = jax.random.uniform(jax.random.fold_in(jax.random.fold_in(rng, 6), dim), (blocks,), jnp.float32, low / len(pieces), high / len(pieces))
        return jnp.repeat(jnp.exp(heights), shape[dim] // blocks).reshape((-1,) + (1,) * (len(shape) - dim - 1))

    loudness = one(*pieces[0])
    for cut in pieces[1:]:
        loudness = loudness * one(*cut)
    return loudness


def shared_out(key, own, number, rows, count, top, most, skew):
    order = jax.random.permutation(key, count)
    packed, common = shares(count, rows * top, most, skew, True), shares(count, rows * top, most, skew, False)
    places = jnp.arange(count)

    def named(tallies, rotation):
        used = int((tallies > 0).sum())
        fixed = max(1, used // 4)
        moved = fixed + (places - fixed + rotation * (used - fixed)) % max(1, count - fixed)
        return jnp.zeros((count,), jnp.int32).at[order[jnp.where(places < fixed, places, moved)]].set(jnp.asarray(tallies, jnp.int32))

    tallies = jnp.where(number % 4 == 0, named(packed, number // 4), named(common, number - number // 4 - 1))
    mixed = jax.random.permutation(jax.random.fold_in(own, 3), count)
    source_of, taker = mixed[0:count // 2 * 2:2], mixed[1:count // 2 * 2:2]
    room = jnp.minimum(tallies[source_of] - 1, most - tallies[taker]) // 2
    room = jnp.where((source_of == order[0]) | (taker == order[0]) | (tallies[taker] == 0), 0, jnp.maximum(room, 0))
    moved = jax.random.randint(jax.random.fold_in(own, 4), (count // 2,), 0, 1 << 20) % (room + 1)
    tallies = tallies.at[source_of].add(-moved).at[taker].add(moved)
    members = jnp.searchsorted(jnp.cumsum(tallies), jnp.arange(rows * top), side="right").astype(jnp.int32)
    table = members.reshape(top, rows).T
    table = table[jax.random.permutation(jax.random.fold_in(own, 1), rows)]
    rotation = jax.random.randint(jax.random.fold_in(own, 2), (rows, 1), 0, top)
    return jnp.take_along_axis(table, (jnp.arange(top)[None, :] + rotation) % top, axis=1)


def shares(count, total, bound, slope, full):
    loads = [(1 << 20) // math.isqrt(grade ** slope) + 1 for grade in range(1, count + 1)]
    largest = bound if full else min(bound, max(-(-total // count), total * loads[0] // sum(loads)))
    least = 1 if total - largest >= count - 1 else 0
    holding, spare = [largest] + [least] * (count - 1), total - largest - least * (count - 1)
    while spare > 0:
        free = [i for i in range(1, count) if holding[i] < largest] or [i for i in range(1, count) if holding[i] < bound]
        pool, remaining = sum([loads[i] for i in free]), spare
        for i in free:
            addition = min(bound - holding[i], max(1, remaining * loads[i] // pool), spare)
            holding[i] = holding[i] + addition
            spare = spare - addition
    return np.array(holding)


def bell_draw(key, shape, width, limit, cuts=(), held_as=jnp.bfloat16):
    loudness = level_of(key, shape, cuts, -0.22, 0.18) if cuts else 1.0
    values = jax.random.normal(key, shape, jnp.float32) * width * loudness
    return jnp.minimum(jnp.maximum(values, -limit), limit).astype(held_as)


def noise_with(key, dims, deviation, reach, pieces, heavy, kind=jnp.bfloat16):
    array = deviation * jax.random.normal(key, dims, jnp.float32)
    if pieces:
        array = array * level_of(key, dims, pieces, -0.22, 0.18)
    return jnp.clip(with_spikes(array, jax.random.fold_in(key, 3), *heavy), -reach, reach).astype(kind)


def setup_inputs(seed: int = 0) -> dict:
    splits = jax.random.split(jax.random.key(seed), 15)
    cotangent = noise_with(splits[0], (SEQUENCE_TOKENS, D), 1.0, 6.0, ((0, 8),), (0, 1, 8, 2.0))
    moe_input = bell_draw(splits[1], (SEQUENCE_TOKENS, D), 1.0, 6.0, ((0, 8),))
    expert_ids_keys = jax.random.split(jax.random.fold_in(splits[2], 1), SEQUENCE_TOKENS // TOK_DEV)
    expert_ids_turns = jax.random.permutation(jax.random.fold_in(splits[2], 3), SEQUENCE_TOKENS // TOK_DEV)
    expert_ids = jax.vmap(lambda own, number: shared_out(jax.random.fold_in(splits[2], 2), own, number, TOK_DEV, EXPERTS, TOP, CAP, 1))(expert_ids_keys, expert_ids_turns).reshape((SEQUENCE_TOKENS, TOP))
    group_weight = jnp.clip(0.3 + 0.7 * jax.random.uniform(splits[3], (SEQUENCE_TOKENS,), jnp.float32) ** level_of(splits[3], (SEQUENCE_TOKENS,), ((0, 8),), -0.2, 0.2), 0.3, 1.0)
    expert_weight = jnp.clip(0.1 + 0.79999997 * jax.random.uniform(splits[4], (SEQUENCE_TOKENS, TOP), jnp.float32) ** level_of(splits[4], (SEQUENCE_TOKENS, TOP), ((0, 8),), -0.2, 0.2), 0.1, 0.9)
    mixer_out = bell_draw(splits[5], (SEQUENCE_TOKENS, RETENTION_HEADS * VD), 1.0, 6.0, ((0, 8), (1, 4)))
    queries = bell_draw(splits[6], (RETENTION_HEADS * KD, SEQUENCE_TOKENS), 1.0, 6.0, ((0, 4), (1, 8)))
    key_vectors = bell_draw(splits[7], (RETENTION_HEADS * KD, SEQUENCE_TOKENS), 1.0, 6.0, ((0, 4), (1, 8)))
    value_vectors = bell_draw(splits[8], (RETENTION_HEADS * VD, SEQUENCE_TOKENS), 1.0, 6.0, ((0, 4), (1, 8)))
    decay_rates = draw_decay_rates(jax.random.fold_in(splits[14], 71), 0)
    proj_weight = bell_draw(splits[10], (D, RETENTION_HEADS * VD), (RETENTION_HEADS * VD) ** -0.5, 0.25, ((1, 4),))
    gate_weight = bell_draw(splits[11], (EXPERTS, D, FF), D ** -0.5, 0.125, ((0, 8), (2, 4)))
    up_weight = bell_draw(splits[12], (EXPERTS, D, FF), D ** -0.5, 0.125, ((0, 8), (2, 4)))
    down_weight = bell_draw(splits[13], (EXPERTS, FF, D), FF ** -0.5, 0.125, ((0, 8), (1, 4)))
    return dict(cotangent=cotangent, moe_input=moe_input, expert_ids=expert_ids, group_weight=group_weight, expert_weight=expert_weight, mixer_out=mixer_out, queries=queries, key_vectors=key_vectors, value_vectors=value_vectors, decay_rates=decay_rates, proj_weight=proj_weight, gate_weight=gate_weight, up_weight=up_weight, down_weight=down_weight)


def slot_table(block_ids, experts_all, capacity):
    flat_ids = block_ids.reshape(-1).astype(jnp.int32)
    expert_range = jnp.arange(experts_all, dtype=jnp.int32)
    onehot = (flat_ids[:, None] == expert_range[None, :]).astype(jnp.int32)
    before = jnp.cumsum(onehot, axis=0) - onehot
    rank_in = jnp.sum(before * onehot, axis=1)
    slot_ids = flat_ids * capacity + rank_in
    slot_range = jnp.arange(experts_all * capacity, dtype=jnp.int32)
    entry_numbers = jnp.arange(1, flat_ids.shape[0] + 1, dtype=jnp.int32)
    owners = jnp.sum(jnp.where(slot_ids[None, :] == slot_range[:, None], entry_numbers[None, :], 0), axis=1) - 1
    return slot_ids, owners


def pack_rows(cotangent, moe_input, group_weight, expert_weight, expert_ids, experts_all, capacity):
    slot_ids, owners = slot_table(expert_ids, experts_all, capacity)
    present = owners >= 0
    entry_ids = jnp.maximum(owners, 0)
    token_ids = entry_ids // expert_ids.shape[1]
    route_weight = (group_weight[:, None] * expert_weight).reshape(-1)
    row_scale = jnp.where(present, route_weight[entry_ids], 0.0)
    cot_rows = (cotangent[token_ids].astype(jnp.float32) * row_scale[:, None]).astype(jnp.bfloat16)
    inp_rows = jnp.where(present[:, None], moe_input[token_ids], jnp.zeros((), moe_input.dtype))
    return cot_rows, inp_rows, slot_ids


def expert_grads(operands):
    rows_cot, rows_inp, w_gate, w_up, w_down = operands
    gate_pre = jnp.dot(rows_inp, w_gate, preferred_element_type=jnp.float32)
    up_pre = jnp.dot(rows_inp, w_up, preferred_element_type=jnp.float32)
    sigmoid_gate = jax.nn.sigmoid(gate_pre)
    hidden = (gate_pre * sigmoid_gate * up_pre).astype(jnp.bfloat16)
    grad_down = jnp.dot(hidden.T, rows_cot, preferred_element_type=jnp.float32).astype(jnp.bfloat16)
    hidden_grad = jnp.dot(rows_cot, w_down.T, preferred_element_type=jnp.float32)
    gate_grad = (hidden_grad * up_pre * sigmoid_gate * (1.0 + gate_pre * (1.0 - sigmoid_gate))).astype(jnp.bfloat16)
    up_grad = (hidden_grad * gate_pre * sigmoid_gate).astype(jnp.bfloat16)
    grad_gate = jnp.dot(rows_inp.T, gate_grad, preferred_element_type=jnp.float32).astype(jnp.bfloat16)
    grad_up = jnp.dot(rows_inp.T, up_grad, preferred_element_type=jnp.float32).astype(jnp.bfloat16)
    entry_sum = jnp.dot(gate_grad, w_gate.T, preferred_element_type=jnp.float32) + jnp.dot(up_grad, w_up.T, preferred_element_type=jnp.float32)
    entry_grad = entry_sum.astype(jnp.bfloat16)
    return grad_gate, grad_up, grad_down, entry_grad


def head_grads(operands):
    query_head, key_head, value_head, grad_head, rate_head = operands
    exact_result = lax.Precision.HIGHEST
    cumulative = jnp.cumsum(rate_head)
    mixing = jnp.exp(-jnp.abs(cumulative[:, None] - cumulative[None, :]))
    score_scale = KD ** -0.5
    scores = score_scale * jnp.dot(query_head.T, key_head, precision=exact_result) * mixing
    score_grad = score_scale * jnp.dot(grad_head.T, value_head, precision=exact_result) * mixing
    query_grad = jnp.dot(key_head, score_grad.T, precision=exact_result)
    key_grad = jnp.dot(query_head, score_grad, precision=exact_result)
    value_grad = jnp.dot(grad_head, scores, precision=exact_result)
    return query_grad, key_grad, value_grad


def reference(cotangent, moe_input, expert_ids, group_weight, expert_weight, mixer_out, queries, key_vectors, value_vectors, decay_rates, proj_weight, gate_weight, up_weight, down_weight):
    packer = jax.vmap(partial(pack_rows, experts_all=EXPERTS, capacity=CAP))
    cot_rows, inp_rows, slot_ids = packer(cotangent.reshape(N_SP, TOK_DEV, D), moe_input.reshape(N_SP, TOK_DEV, D), group_weight.reshape(N_SP, TOK_DEV), expert_weight.reshape(N_SP, TOK_DEV, TOP), expert_ids.reshape(N_SP, TOK_DEV, TOP))

    def by_expert(rows):
        return rows.reshape(N_SP, EXPERTS, CAP, D).transpose(1, 0, 2, 3).reshape(EXPERTS, N_SP * CAP, D)

    grad_gate, grad_up, grad_down, entry_grad = lax.map(expert_grads, (by_expert(cot_rows), by_expert(inp_rows), gate_weight, up_weight, down_weight))
    returned = entry_grad.reshape(EXPERTS, N_SP, CAP, D).transpose(1, 0, 2, 3).reshape(N_SP, EXPERTS * CAP, D)

    def pick_rows(rows, indices):
        return rows[indices]

    picked = jax.vmap(pick_rows)(returned, slot_ids)
    moe_grad = jnp.sum(picked.astype(jnp.float32).reshape(SEQUENCE_TOKENS, TOP, D), axis=1)
    resid_grad = (cotangent.astype(jnp.float32) + moe_grad).astype(jnp.bfloat16)
    grad_proj = jnp.dot(resid_grad.T, mixer_out, preferred_element_type=jnp.float32)
    out_grad = jnp.dot(proj_weight.T, resid_grad.T, preferred_element_type=jnp.float32)
    query_heads = queries.astype(jnp.float32).reshape(RETENTION_HEADS, KD, SEQUENCE_TOKENS)
    key_heads = key_vectors.astype(jnp.float32).reshape(RETENTION_HEADS, KD, SEQUENCE_TOKENS)
    value_heads = value_vectors.astype(jnp.float32).reshape(RETENTION_HEADS, VD, SEQUENCE_TOKENS)
    grad_heads = out_grad.reshape(RETENTION_HEADS, VD, SEQUENCE_TOKENS)
    query_grad, key_grad, value_grad = lax.map(head_grads, (query_heads, key_heads, value_heads, grad_heads, decay_rates))
    return (grad_gate, grad_up, grad_down, grad_proj, query_grad.reshape(RETENTION_HEADS * KD, SEQUENCE_TOKENS), key_grad.reshape(RETENTION_HEADS * KD, SEQUENCE_TOKENS), value_grad.reshape(RETENTION_HEADS * VD, SEQUENCE_TOKENS))
```

```python
import functools

import jax
import jax.numpy as jnp
from jax import lax
from jax.experimental import pallas as pl
from jax.experimental.pallas import tpu as pltpu
from jax.sharding import PartitionSpec as P

MESH = pl.DeviceIdType.MESH
VMEM = pl.BlockSpec(memory_space=pltpu.VMEM)
ANY = pl.BlockSpec(memory_space=pl.ANY)


def partner(place, k, count):
    if k == 0:
        return place
    out = 0
    bit = 1
    while bit < count:
        b = lax.rem(place // bit, 2)
        out = out + bit * ((1 - b) if k & bit else b)
        bit *= 2
    return out


def remote(src, dst, send_sem, recv_sem, sp_place, tp_place):
    return pltpu.make_async_remote_copy(
        src_ref=src,
        dst_ref=dst,
        send_sem=send_sem,
        recv_sem=recv_sem,
        device_id={"sp": sp_place, "tp": tp_place},
        device_id_type=MESH,
    )


def state_side(here, there, count):
    return (here + count - there) // count


def dot(a, b, a_dim, b_dim):
    return lax.dot_general(
        a, b, (((a_dim,), (b_dim,)), ((), ())), preferred_element_type=jnp.float32
    )


def experts_kernel(
    sp_count, tp_count, groups,
    ids, group, weight, rates, keys, values, cot_hbm, inp_hbm, gate_hbm, up_hbm, down_hbm,
    resid, state_all, grad_gate, grad_up, grad_down,
    cot, inp, w_gate, w_up, w_down, picks, either, scaled, z_src, pair_src, rows, state,
    hidden, gate_grad, up_grad, part, own_part, summed_in, outgoing, returned,
    load_sem, send_z, recv_z, send_xy, recv_xy, send_far, recv_far, send_state, recv_state,
    send_rs, recv_rs, send_back, recv_back, send_ag, recv_ag,
):
    me = lax.axis_index("sp")
    q = lax.axis_index("tp")
    tokens, model_width = cot.shape
    width = model_width // tp_count
    block_rows = rows.shape[2]
    hidden_width = w_gate.shape[1]
    square = tp_count == 4
    at = [partner(me, k, sp_count) for k in range(sp_count)]
    peer = [partner(q, m, tp_count) for m in range(tp_count)]

    def columns(place):
        return pl.ds(pl.multiple_of(place * width, width), width)

    mine = columns(q)
    loads = []
    for i, (src, dst) in enumerate(
        (
            (cot_hbm, cot),
            (inp_hbm, inp),
            (gate_hbm.at[0], w_gate),
            (up_hbm.at[0], w_up),
            (down_hbm.at[0], w_down),
        )
    ):
        copy = pltpu.make_async_copy(src, dst, load_sem.at[i])
        copy.start()
        loads.append(copy)

    barrier = pltpu.get_barrier_semaphore()
    for k in range(1, sp_count):
        pl.semaphore_signal(
            barrier, inc=1, device_id={"sp": at[k], "tp": q}, device_id_type=MESH
        )
    for m in range(1, tp_count):
        pl.semaphore_signal(
            barrier, inc=1, device_id={"sp": me, "tp": peer[m]}, device_id_type=MESH
        )

    top_count = ids.shape[0]
    expert = lax.broadcasted_iota(jnp.int32, (sp_count, tokens), 0)
    named = [(ids[j : j + 1, :] == expert).astype(jnp.float32) for j in range(top_count)]
    earlier = lax.broadcasted_iota(jnp.int32, (tokens, tokens), 0) < lax.broadcasted_iota(
        jnp.int32, (tokens, tokens), 1
    )
    before = jnp.dot(
        sum(named).astype(jnp.bfloat16),
        earlier.astype(jnp.float32).astype(jnp.bfloat16),
        preferred_element_type=jnp.float32,
    )
    slots = []
    route = jnp.zeros((8, tokens), jnp.float32)
    lane_of = lax.broadcasted_iota(jnp.int32, (8, tokens), 0)
    for j in range(top_count):
        rank = jnp.sum(named[j] * before, axis=0, keepdims=True).astype(jnp.int32)
        before = before + named[j]
        slots.append(ids[j : j + 1, :] * block_rows + rank)
        route = jnp.where(lane_of == j, group[...] * weight[j : j + 1, :], route)
    route = jnp.transpose(route)
    row_of = lax.broadcasted_iota(jnp.int32, (block_rows, tokens), 0)
    for k in range(sp_count):
        here = pl.ds(k * block_rows, block_rows)
        pick = [(s == row_of + at[k] * block_rows).astype(jnp.float32) for s in slots]
        for j in range(top_count):
            picks[here, j * tokens : (j + 1) * tokens] = pick[j].astype(jnp.bfloat16)
        either[here, :] = sum(pick).astype(jnp.bfloat16)

    loads[0].wait()
    loads[1].wait()
    cot_mine = cot[:, mine].astype(jnp.float32)
    scaled_mine = jnp.concatenate(
        [(cot_mine * route[:, j : j + 1]).astype(jnp.bfloat16) for j in range(top_count)], axis=0
    )
    first = 2 * block_rows
    cot_out = jnp.dot(picks[first:, :], scaled_mine, preferred_element_type=jnp.float32)
    inp_out = jnp.dot(either[first:, :], inp[:, mine], preferred_element_type=jnp.float32)
    for k in range(2, sp_count):
        here = slice((k - 2) * block_rows, (k - 1) * block_rows)
        z_src[k, 0] = cot_out[here].astype(z_src.dtype)
        z_src[k, 1] = inp_out[here].astype(z_src.dtype)
    pl.semaphore_wait(barrier, sp_count - 1 + tp_count - 1)

    waits = []

    def send(copy):
        copy.start()
        waits.append(copy)

    for k in range(2, sp_count):
        send(remote(z_src.at[k], rows.at[:, k, :, mine], send_z.at[k], recv_z.at[k], at[k], q))

    cot_all = cot[...].astype(jnp.float32)
    for j in range(top_count):
        scaled[j * tokens : (j + 1) * tokens, :] = (cot_all * route[:, j : j + 1]).astype(scaled.dtype)
    cot_out = jnp.dot(picks[:first, :], scaled[...], preferred_element_type=jnp.float32)
    inp_out = jnp.dot(either[:first, :], inp[...], preferred_element_type=jnp.float32)
    pair_src[0] = cot_out[block_rows:].astype(pair_src.dtype)
    pair_src[1] = inp_out[block_rows:].astype(pair_src.dtype)
    send(remote(pair_src, rows.at[:, 1], send_z.at[1], recv_z.at[1], at[1], q))
    rows[0, 0] = cot_out[:block_rows].astype(rows.dtype)
    rows[1, 0] = inp_out[:block_rows].astype(rows.dtype)

    exact = lax.Precision.HIGHEST
    heads, length = rates.shape
    key_size = keys.shape[0] // heads
    value_size = values.shape[0] // heads
    upto = lax.broadcasted_iota(jnp.int32, (length, length), 0) <= lax.broadcasted_iota(
        jnp.int32, (length, length), 1
    )
    for h in range(heads):
        rate = jnp.broadcast_to(rates[h : h + 1, :], (8, length))
        prefix = jnp.dot(
            rate, upto.astype(jnp.float32), precision=exact, preferred_element_type=jnp.float32
        )[0:1]
        ending = prefix[:, length - 1 : length]
        key = keys[h * key_size : (h + 1) * key_size, :].astype(jnp.float32)
        value = values[h * value_size : (h + 1) * value_size, :].astype(jnp.float32)
        top = h * (key_size + 8)
        for side, reach in enumerate((jnp.exp(prefix - ending), jnp.exp(-prefix))):
            state[side, top : top + key_size, :] = lax.dot_general(
                key * reach,
                value,
                (((1,), (1,)), ((), ())),
                precision=exact,
                preferred_element_type=jnp.float32,
            )
            state[side, top + key_size : top + key_size + 8, :] = jnp.broadcast_to(
                ending, (8, value_size)
            )
    state_all[me] = state[0]
    for k in range(1, sp_count):
        send(
            remote(
                state.at[state_side(me, at[k], sp_count)],
                state_all.at[me],
                send_state.at[k],
                recv_state.at[k],
                at[k],
                q,
            )
        )

    def land(g):
        for k in range(*groups[g]):
            if k < 2:
                continue
            piece = rows.at[:, k, :, mine]
            remote(z_src.at[k], piece, send_z.at[k], recv_z.at[k], me, q).wait_recv()
            for m in range(1, tp_count):
                if square and m == 3:
                    continue
                send(
                    remote(piece, piece, send_xy.at[k, m - 1], recv_xy.at[k, m - 1], me, peer[m])
                )

    def relay(g):
        for k in range(*groups[g]):
            if k < 2:
                continue
            for m in range(1, tp_count):
                if square and m == 3:
                    continue
                piece = rows.at[:, k, :, columns(peer[m])]
                remote(piece, piece, send_xy.at[k, m - 1], recv_xy.at[k, m - 1], me, q).wait_recv()
                if square:
                    a = m - 1
                    half = rows.at[a, k, :, columns(peer[m])]
                    send(
                        remote(half, half, send_far.at[a, k], recv_far.at[a, k], me, peer[3 - m])
                    )

    def settle(g):
        for k in range(*groups[g]):
            if k == 1:
                remote(pair_src, rows.at[:, 1], send_z.at[1], recv_z.at[1], me, q).wait_recv()
            if k >= 2 and square:
                for a in range(2):
                    piece = rows.at[a, k, :, columns(peer[3])]
                    remote(piece, piece, send_far.at[a, k], recv_far.at[a, k], me, q).wait_recv()

    def forward(g):
        low, high = groups[g]
        count = high - low
        size = count * block_rows
        here = slice(low * block_rows, high * block_rows)
        got = rows[1, low:high].reshape(size, model_width)
        gate_pre = jnp.dot(got, w_gate[...], preferred_element_type=jnp.float32)
        up_pre = jnp.dot(got, w_up[...], preferred_element_type=jnp.float32)
        sigmoid_gate = jax.nn.sigmoid(gate_pre)
        silu_gate = gate_pre * sigmoid_gate
        hidden[here, :] = (silu_gate * up_pre).astype(hidden.dtype)
        got = rows[0, low:high].reshape(size, model_width)
        hidden_grad = dot(got, w_down[...], 1, 1)
        gate_rows = (
            hidden_grad * up_pre * sigmoid_gate * (1.0 + gate_pre * (1.0 - sigmoid_gate))
        ).astype(jnp.bfloat16)
        up_rows = (hidden_grad * silu_gate).astype(jnp.bfloat16)
        gate_grad[here, :] = gate_rows
        up_grad[here, :] = up_rows
        for m in list(range(tp_count - 1, 0, -1)) + [0]:
            theirs = columns(peer[m])
            partial = dot(gate_rows, w_gate[theirs, :], 1, 1) + dot(up_rows, w_up[theirs, :], 1, 1)
            partial = partial.reshape(count, block_rows, width)
            if m == 0:
                own_part[low:high] = partial
            else:
                part[m - 1, low:high] = partial.astype(part.dtype)
                send(
                    remote(
                        part.at[m - 1, pl.ds(low, count)],
                        summed_in.at[m - 1, pl.ds(low, count)],
                        send_rs.at[g, m - 1],
                        recv_rs.at[g, m - 1],
                        me,
                        peer[m],
                    )
                )

    def give_back(g):
        low, high = groups[g]
        count = high - low
        total = own_part[low:high]
        for m in range(1, tp_count):
            piece = summed_in.at[m - 1, pl.ds(low, count)]
            remote(piece, piece, send_rs.at[g, m - 1], recv_rs.at[g, m - 1], me, q).wait_recv()
            total = total + summed_in[m - 1, low:high].astype(jnp.float32)
        total = total.astype(outgoing.dtype)
        for k in range(low, high):
            if k == 0:
                returned[0] = total[0]
            else:
                outgoing[k] = total[k - low]
                send(
                    remote(
                        outgoing.at[k], returned.at[k], send_back.at[k], recv_back.at[k], at[k], q
                    )
                )

    all_rows = sp_count * block_rows

    def down_grads():
        got = rows[0].reshape(all_rows, model_width)
        for m in range(tp_count):
            cut = slice(m * width, (m + 1) * width)
            grad_down[:, cut] = dot(hidden[...], got[:, cut], 0, 0).astype(grad_down.dtype)

    def input_grads(grads, out):
        for m in range(tp_count):
            cut = slice(m * width, (m + 1) * width)
            got = rows[1, :, :, cut].reshape(all_rows, width)
            out[cut, :] = dot(got, grads[...], 0, 0).astype(out.dtype)

    count = len(groups)
    land(0)
    land(1)
    relay(0)
    for load in loads[2:]:
        load.wait()
    settle(0)
    forward(0)
    for g in range(1, count):
        relay(g)
        if g + 1 < count:
            land(g + 1)
        elif g >= 2:
            give_back(0)
        settle(g)
        forward(g)
    for g in range(0 if count <= 2 else 1, count - 1):
        give_back(g)
    down_grads()
    give_back(count - 1)
    input_grads(gate_grad, grad_gate)
    for k in range(1, sp_count):
        remote(
            outgoing.at[k], returned.at[k], send_back.at[k], recv_back.at[k], me, q
        ).wait_recv()
    total = dot(either[...], returned[...].reshape(all_rows, width), 0, 0)
    resid[:, mine] = (cot[:, mine].astype(jnp.float32) + total).astype(resid.dtype)
    piece = resid.at[:, mine]
    for m in range(tp_count - 1, 0, -1):
        send(remote(piece, piece, send_ag.at[m - 1], recv_ag.at[m - 1], me, peer[m]))
    input_grads(up_grad, grad_up)
    for m in range(1, tp_count):
        piece = resid.at[:, columns(peer[m])]
        remote(piece, piece, send_ag.at[m - 1], recv_ag.at[m - 1], me, q).wait_recv()
    for k in range(1, sp_count):
        piece = state_all.at[at[k]]
        remote(piece, piece, send_state.at[k], recv_state.at[k], me, q).wait_recv()
    for copy in waits:
        copy.wait_send()


def experts(
    ids, group, weight, rates, keys, values, cot, inp, gate, up, down, capacity, sp_count, tp_count
):
    tokens, model_width = cot.shape
    width = model_width // tp_count
    hidden_width = gate.shape[2]
    heads = rates.shape[0]
    state_rows = keys.shape[0] + 8 * heads
    value_size = values.shape[0] // heads
    block_rows = -(-capacity // 16) * 16
    all_rows = sp_count * block_rows
    quarter = sp_count // 4
    groups = [(i * quarter, (i + 1) * quarter) for i in range(4)]
    kind = cot.dtype
    dma = pltpu.SemaphoreType.DMA
    vmem = pltpu.VMEM
    return pl.pallas_call(
        functools.partial(experts_kernel, sp_count, tp_count, groups),
        out_shape=(
            jax.ShapeDtypeStruct((tokens, model_width), kind),
            jax.ShapeDtypeStruct((sp_count, state_rows, value_size), jnp.float32),
            jax.ShapeDtypeStruct((model_width, hidden_width), kind),
            jax.ShapeDtypeStruct((model_width, hidden_width), kind),
            jax.ShapeDtypeStruct((hidden_width, model_width), kind),
        ),
        in_specs=[VMEM] * 6 + [ANY] * 5,
        out_specs=(VMEM,) * 5,
        scratch_shapes=[
            vmem((tokens, model_width), kind),
            vmem((tokens, model_width), kind),
            vmem((model_width, hidden_width), kind),
            vmem((model_width, hidden_width), kind),
            vmem((hidden_width, model_width), kind),
            vmem((all_rows, ids.shape[0] * tokens), jnp.bfloat16),
            vmem((all_rows, tokens), jnp.bfloat16),
            vmem((ids.shape[0] * tokens, model_width), kind),
            vmem((sp_count, 2, block_rows, width), kind),
            vmem((2, block_rows, model_width), kind),
            vmem((2, sp_count, block_rows, model_width), kind),
            vmem((2, state_rows, value_size), jnp.float32),
            vmem((all_rows, hidden_width), kind),
            vmem((all_rows, hidden_width), kind),
            vmem((all_rows, hidden_width), kind),
            vmem((tp_count - 1, sp_count, block_rows, width), kind),
            vmem((sp_count, block_rows, width), jnp.float32),
            vmem((tp_count - 1, sp_count, block_rows, width), kind),
            vmem((sp_count, block_rows, width), kind),
            vmem((sp_count, block_rows, width), kind),
            dma((5,)),
            dma((sp_count,)),
            dma((sp_count,)),
            dma((sp_count, tp_count - 1)),
            dma((sp_count, tp_count - 1)),
            dma((2, sp_count)),
            dma((2, sp_count)),
            dma((sp_count,)),
            dma((sp_count,)),
            dma((len(groups), tp_count - 1)),
            dma((len(groups), tp_count - 1)),
            dma((sp_count,)),
            dma((sp_count,)),
            dma((tp_count - 1,)),
            dma((tp_count - 1,)),
        ],
        compiler_params=pltpu.CompilerParams(
            collective_id=0, has_side_effects=True, vmem_limit_bytes=60 * 1024 * 1024
        ),
    )(ids, group, weight, rates, keys, values, cot, inp, gate, up, down)


def on_device(
    cotangent,
    moe_input,
    expert_ids,
    group_weight,
    expert_weight,
    mixer_out,
    queries,
    key_vectors,
    value_vectors,
    decay_rates,
    proj_weight,
    gate_weight,
    up_weight,
    down_weight,
):
    exact = lax.Precision.HIGHEST
    sp_count = lax.axis_size("sp")
    tp_count = lax.axis_size("tp")
    me = lax.axis_index("sp")
    local_experts = gate_weight.shape[0]
    experts_all = local_experts * sp_count
    rows_here, model_width = cotangent.shape
    top_count = expert_ids.shape[1]
    capacity = 3 * top_count * rows_here // (2 * experts_all)

    heads_here, length = decay_rates.shape
    query_full = queries.astype(jnp.float32).reshape(heads_here, -1, length)
    key_full = key_vectors.astype(jnp.float32).reshape(heads_here, -1, length)
    value_full = value_vectors.astype(jnp.float32).reshape(heads_here, -1, length)
    key_size = query_full.shape[1]
    value_size = value_full.shape[1]
    score_scale = key_size ** (-0.5)
    place = jnp.arange(length, dtype=jnp.int32)
    prefix = jnp.dot(
        decay_rates, (place[:, None] <= place[None, :]).astype(jnp.float32), precision=exact
    )
    ending = prefix[:, -1:]
    mixing = score_scale * jnp.exp(-jnp.abs(prefix[:, :, None] - prefix[:, None, :]))
    toward_end = jnp.exp(prefix - ending)
    from_start = jnp.exp(-prefix)
    both_weights = jnp.stack([toward_end, from_start])
    resid_grad, key_states, grad_gate, grad_up, grad_down = experts(
        expert_ids.T,
        group_weight[None, :],
        expert_weight.T,
        decay_rates,
        key_vectors,
        value_vectors,
        cotangent,
        moe_input,
        gate_weight,
        up_weight,
        down_weight,
        capacity,
        sp_count,
        tp_count,
    )
    grad_gate, grad_up, grad_down = grad_gate[None], grad_up[None], grad_down[None]
    key_states = key_states.reshape(sp_count, heads_here, -1, value_size)

    proj_part = lax.dot_general(
        resid_grad, mixer_out, (((0,), (0,)), ((), ())), preferred_element_type=jnp.float32
    ).astype(jnp.bfloat16)
    out_grad = lax.dot_general(
        proj_weight, resid_grad, (((0,), (1,)), ((), ())), preferred_element_type=jnp.float32
    ).reshape(heads_here, -1, length)
    query_state = jnp.einsum(
        "whkl,hvl->whkv", query_full[None] * both_weights[:, :, None, :], out_grad, precision=exact
    )
    block = jnp.arange(sp_count, dtype=jnp.int32)
    query_state = query_state.astype(jnp.bfloat16).transpose(0, 2, 1, 3)
    query_state = query_state.reshape(2, key_size, heads_here * value_size)
    sent = jnp.concatenate(
        [
            proj_part.reshape(sp_count, -1, heads_here * value_size),
            jnp.where((block > me)[:, None, None], query_state[:1], query_state[1:]),
        ],
        axis=1,
    )
    shared = lax.all_to_all(sent, "sp", split_axis=0, concat_axis=0, tiled=True)
    shared = shared.astype(jnp.float32)
    proj_rows = model_width // sp_count
    grad_proj = jnp.sum(shared[:, :proj_rows], axis=0)
    query_states = shared[:, proj_rows:].reshape(sp_count, key_size, heads_here, value_size)
    query_states = query_states.transpose(0, 2, 1, 3)

    totals = key_states[:, :, key_size, 0]
    low_between = (block[None, :] > block[:, None]) & (block[None, :] < me)
    high_between = (block[None, :] < block[:, None]) & (block[None, :] > me)
    low_decay = jnp.exp(-jnp.sum(jnp.where(low_between[:, :, None], totals[None], 0.0), axis=1))
    high_decay = jnp.exp(-jnp.sum(jnp.where(high_between[:, :, None], totals[None], 0.0), axis=1))
    low_decay = jnp.where((block < me)[:, None], low_decay, 0.0)
    high_decay = jnp.where((block > me)[:, None], high_decay, 0.0)
    both_decays = jnp.stack([low_decay, high_decay])[:, :, :, None, None]
    key_carried = jnp.sum(both_decays * key_states[None, :, :, :key_size], axis=1)
    query_carried = jnp.sum(both_decays * query_states[None], axis=1)

    scores = mixing * jnp.einsum("hkt,hks->hts", query_full, key_full, precision=exact)
    score_grad = mixing * jnp.einsum("hvt,hvs->hts", out_grad, value_full, precision=exact)
    query_grad = jnp.einsum("hks,hts->hkt", key_full, score_grad, precision=exact)
    key_grad = jnp.einsum("hkt,hts->hks", query_full, score_grad, precision=exact)
    value_grad = jnp.einsum("hvt,hts->hvs", out_grad, scores, precision=exact)
    reach = score_scale * jnp.stack([from_start, toward_end])
    out_reach = out_grad[None] * reach[:, :, None, :]
    value_reach = value_full[None] * reach[:, :, None, :]
    key_reach = key_full[None] * reach[:, :, None, :]
    query_grad = query_grad + jnp.einsum("whvl,whkv->hkl", out_reach, key_carried, precision=exact)
    key_grad = key_grad + jnp.einsum("whvl,whkv->hkl", value_reach, query_carried, precision=exact)
    value_grad = value_grad + jnp.einsum("whkl,whkv->hvl", key_reach, query_carried, precision=exact)
    return (
        grad_gate,
        grad_up,
        grad_down,
        grad_proj,
        query_grad.reshape(heads_here * key_size, length),
        key_grad.reshape(heads_here * key_size, length),
        value_grad.reshape(heads_here * value_size, length),
    )


def solution(mesh):
    return jax.shard_map(
        on_device,
        mesh=mesh,
        in_specs=(
            P("sp", None),
            P("sp", None),
            P("sp", None),
            P("sp"),
            P("sp", None),
            P("sp", "tp"),
            P("tp", "sp"),
            P("tp", "sp"),
            P("tp", "sp"),
            P("tp", "sp"),
            P(None, "tp"),
            P("sp", None, "tp"),
            P("sp", None, "tp"),
            P("sp", "tp", None),
        ),
        out_specs=(
            P("sp", None, "tp"),
            P("sp", None, "tp"),
            P("sp", "tp", None),
            P("sp", "tp"),
            P("tp", "sp"),
            P("tp", "sp"),
            P("tp", "sp"),
        ),
        check_vma=False,
    )
```

```python
import functools

import jax
import jax.numpy as jnp
from jax import lax
from jax.experimental import pallas as pl
from jax.experimental.pallas import tpu as pltpu
from jax.sharding import PartitionSpec as P

MESH = pl.DeviceIdType.MESH
VMEM = pl.BlockSpec(memory_space=pltpu.VMEM)
ANY = pl.BlockSpec(memory_space=pl.ANY)


def partner(place, k, count):
    if k == 0:
        return place
    out = 0
    bit = 1
    while bit < count:
        b = lax.rem(place // bit, 2)
        out = out + bit * ((1 - b) if k & bit else b)
        bit *= 2
    return out


def remote(src, dst, send_sem, recv_sem, sp_place, tp_place):
    return pltpu.make_async_remote_copy(
        src_ref=src,
        dst_ref=dst,
        send_sem=send_sem,
        recv_sem=recv_sem,
        device_id={"sp": sp_place, "tp": tp_place},
        device_id_type=MESH,
    )


def state_side(here, there, count):
    return (here + count - there) // count


def dot(a, b, a_dim, b_dim):
    return lax.dot_general(
        a, b, (((a_dim,), (b_dim,)), ((), ())), preferred_element_type=jnp.float32
    )


def experts_kernel(
    sp_count, tp_count, groups,
    ids, group, weight, rates, queries, keys, values, mixer, cot_hbm, inp_hbm, gate_hbm, up_hbm, down_hbm, proj_hbm,
    grad_gate, grad_up, grad_down, grad_proj, grad_queries, grad_keys, grad_values,
    cot, inp, w_gate, w_up, w_down, w_proj, picks, either, scaled, z_src, pair_src, rows, state, state_all, resid,
    scores, mixing, reaches, key_carried, proj, pair_in, proj_out, proj_in, query_out, query_all,
    hidden, gate_grad, up_grad, part, own_part, summed_in, outgoing, returned,
    load_sem, send_z, recv_z, send_xy, recv_xy, send_far, recv_far, send_state, recv_state,
    send_rs, recv_rs, send_back, recv_back, send_ag, recv_ag, send_pair, recv_pair, send_proj, recv_proj,
    send_query, recv_query,
):
    me = lax.axis_index("sp")
    q = lax.axis_index("tp")
    tokens, model_width = cot.shape
    width = model_width // tp_count
    block_rows = rows.shape[2]
    hidden_width = w_gate.shape[1]
    square = tp_count == 4
    at = [partner(me, k, sp_count) for k in range(sp_count)]
    peer = [partner(q, m, tp_count) for m in range(tp_count)]

    def columns(place):
        return pl.ds(pl.multiple_of(place * width, width), width)

    mine = columns(q)
    loads = []
    for i, (src, dst) in enumerate(
        (
            (cot_hbm, cot),
            (inp_hbm, inp),
            (gate_hbm.at[0], w_gate),
            (up_hbm.at[0], w_up),
            (down_hbm.at[0], w_down),
            (proj_hbm, w_proj),
        )
    ):
        copy = pltpu.make_async_copy(src, dst, load_sem.at[i])
        copy.start()
        loads.append(copy)

    barrier = pltpu.get_barrier_semaphore()
    for k in range(1, sp_count):
        pl.semaphore_signal(
            barrier, inc=1, device_id={"sp": at[k], "tp": q}, device_id_type=MESH
        )
    for m in range(1, tp_count):
        pl.semaphore_signal(
            barrier, inc=1, device_id={"sp": me, "tp": peer[m]}, device_id_type=MESH
        )

    with jax.named_scope("slots"):
        top_count = ids.shape[0]
        expert = lax.broadcasted_iota(jnp.int32, (sp_count, tokens), 0)
        named = [(ids[j : j + 1, :] == expert).astype(jnp.float32) for j in range(top_count)]
        earlier = lax.broadcasted_iota(jnp.int32, (tokens, tokens), 0) < lax.broadcasted_iota(
            jnp.int32, (tokens, tokens), 1
        )
        before = jnp.dot(
            sum(named).astype(jnp.bfloat16),
            earlier.astype(jnp.float32).astype(jnp.bfloat16),
            preferred_element_type=jnp.float32,
        )
        slots = []
        route = jnp.zeros((8, tokens), jnp.float32)
        lane_of = lax.broadcasted_iota(jnp.int32, (8, tokens), 0)
        for j in range(top_count):
            rank = jnp.sum(named[j] * before, axis=0, keepdims=True).astype(jnp.int32)
            before = before + named[j]
            slots.append(ids[j : j + 1, :] * block_rows + rank)
            route = jnp.where(lane_of == j, group[...] * weight[j : j + 1, :], route)
        route = jnp.transpose(route)
        row_of = lax.broadcasted_iota(jnp.int32, (block_rows, tokens), 0)
        for k in range(sp_count):
            here = pl.ds(k * block_rows, block_rows)
            pick = [(s == row_of + at[k] * block_rows).astype(jnp.float32) for s in slots]
            for j in range(top_count):
                picks[here, j * tokens : (j + 1) * tokens] = pick[j].astype(jnp.bfloat16)
            either[here, :] = sum(pick).astype(jnp.bfloat16)

    with jax.named_scope("pack"):
        loads[0].wait()
        loads[1].wait()
        cot_mine = cot[:, mine].astype(jnp.float32)
        scaled_mine = jnp.concatenate(
            [(cot_mine * route[:, j : j + 1]).astype(jnp.bfloat16) for j in range(top_count)], axis=0
        )
        first = 2 * block_rows
        cot_out = jnp.dot(picks[first:, :], scaled_mine, preferred_element_type=jnp.float32)
        inp_out = jnp.dot(either[first:, :], inp[:, mine], preferred_element_type=jnp.float32)
        for k in range(2, sp_count):
            here = slice((k - 2) * block_rows, (k - 1) * block_rows)
            z_src[k, 0] = cot_out[here].astype(z_src.dtype)
            z_src[k, 1] = inp_out[here].astype(z_src.dtype)
    with jax.named_scope("barrier"):
        pl.semaphore_wait(barrier, sp_count - 1 + tp_count - 1)

    waits = []

    def send(copy):
        copy.start()
        waits.append(copy)

    for k in range(2, sp_count):
        send(remote(z_src.at[k], rows.at[:, k, :, mine], send_z.at[k], recv_z.at[k], at[k], q))

    with jax.named_scope("near"):
        cot_all = cot[...].astype(jnp.float32)
        for j in range(top_count):
            scaled[j * tokens : (j + 1) * tokens, :] = (cot_all * route[:, j : j + 1]).astype(scaled.dtype)
        cot_out = jnp.dot(picks[:first, :], scaled[...], preferred_element_type=jnp.float32)
        inp_out = jnp.dot(either[:first, :], inp[...], preferred_element_type=jnp.float32)
        pair_src[0] = cot_out[block_rows:].astype(pair_src.dtype)
        pair_src[1] = inp_out[block_rows:].astype(pair_src.dtype)
        send(remote(pair_src, rows.at[:, 1], send_z.at[1], recv_z.at[1], at[1], q))
        rows[0, 0] = cot_out[:block_rows].astype(rows.dtype)
        rows[1, 0] = inp_out[:block_rows].astype(rows.dtype)

    exact = lax.Precision.HIGHEST
    heads, length = rates.shape
    key_size = keys.shape[0] // heads
    value_size = values.shape[0] // heads
    score_scale = key_size ** (-0.5)

    def exact_dot(a, b, a_dim, b_dim):
        return lax.dot_general(
            a,
            b,
            (((a_dim,), (b_dim,)), ((), ())),
            precision=exact,
            preferred_element_type=jnp.float32,
        )

    def key_part(h):
        return slice(h * key_size, (h + 1) * key_size)

    def value_part(h):
        return slice(h * value_size, (h + 1) * value_size)

    def reach_part(h, side):
        return slice(8 * h + side, 8 * h + side + 1)

    with jax.named_scope("states"):
        upto = lax.broadcasted_iota(jnp.int32, (length, length), 0) <= lax.broadcasted_iota(
            jnp.int32, (length, length), 1
        )
        for h in range(heads):
            rate = jnp.broadcast_to(rates[h : h + 1, :], (8, length))
            prefixes = exact_dot(rate, upto.astype(jnp.float32), 1, 0)
            prefix = prefixes[0:1]
            ending = prefix[:, length - 1 : length]
            gap = jnp.transpose(prefixes)[:, 0:1] - prefix
            mixing[h] = score_scale * jnp.exp(-jnp.abs(gap))
            key = keys[key_part(h), :].astype(jnp.float32)
            value = values[value_part(h), :].astype(jnp.float32)
            top = h * (key_size + 8)
            for side, reach in enumerate((jnp.exp(prefix - ending), jnp.exp(-prefix))):
                reaches[reach_part(h, side), :] = reach
                state[side, top : top + key_size, :] = exact_dot(key * reach, value, 1, 1)
                state[side, top + key_size : top + key_size + 8, :] = jnp.broadcast_to(
                    ending, (8, value_size)
                )
        state_all[me] = state[0]
        query_all[me] = jnp.zeros(query_all.shape[1:], query_all.dtype)
        for k in range(1, sp_count):
            send(
                remote(
                    state.at[state_side(me, at[k], sp_count)],
                    state_all.at[me],
                    send_state.at[k],
                    recv_state.at[k],
                    at[k],
                    q,
                )
            )

    def score_stage():
        for h in range(heads):
            query = queries[key_part(h), :].astype(jnp.float32)
            key = keys[key_part(h), :].astype(jnp.float32)
            scores[h] = mixing[h] * exact_dot(query, key, 0, 0)

    def decays(h):
        total_at = h * (key_size + 8) + key_size
        low, high = [None] * sp_count, [None] * sp_count
        totals = [state_all[b, total_at : total_at + 1, :] for b in range(sp_count)]
        run = jnp.zeros((1, value_size), jnp.float32)
        for b in reversed(range(sp_count)):
            low[b] = jnp.where(b < me, jnp.exp(-run), 0.0)
            run = run + jnp.where(b < me, totals[b], 0.0)
        run = jnp.zeros((1, value_size), jnp.float32)
        for b in range(sp_count):
            high[b] = jnp.where(b > me, jnp.exp(-run), 0.0)
            run = run + jnp.where(b > me, totals[b], 0.0)
        return low, high

    def carry_stage():
        for k in range(1, sp_count):
            piece = state_all.at[at[k]]
            remote(piece, piece, send_state.at[k], recv_state.at[k], me, q).wait_recv()
        for h in range(heads):
            top = h * (key_size + 8)
            for side, decay in enumerate(decays(h)):
                total = jnp.zeros((key_size, value_size), jnp.float32)
                for b in range(sp_count):
                    total = total + decay[b] * state_all[b, top : top + key_size, :]
                key_carried[h, :, side * value_size : (side + 1) * value_size] = total

    def land(g):
        for k in range(*groups[g]):
            if k < 2:
                continue
            piece = rows.at[:, k, :, mine]
            remote(z_src.at[k], piece, send_z.at[k], recv_z.at[k], me, q).wait_recv()
            for m in range(1, tp_count):
                if square and m == 3:
                    continue
                send(
                    remote(piece, piece, send_xy.at[k, m - 1], recv_xy.at[k, m - 1], me, peer[m])
                )

    def relay(g):
        for k in range(*groups[g]):
            if k < 2:
                continue
            for m in range(1, tp_count):
                if square and m == 3:
                    continue
                piece = rows.at[:, k, :, columns(peer[m])]
                remote(piece, piece, send_xy.at[k, m - 1], recv_xy.at[k, m - 1], me, q).wait_recv()
                if square:
                    a = m - 1
                    half = rows.at[a, k, :, columns(peer[m])]
                    send(
                        remote(half, half, send_far.at[a, k], recv_far.at[a, k], me, peer[3 - m])
                    )

    def settle(g):
        for k in range(*groups[g]):
            if k == 1:
                remote(pair_src, rows.at[:, 1], send_z.at[1], recv_z.at[1], me, q).wait_recv()
            if k >= 2 and square:
                for a in range(2):
                    piece = rows.at[a, k, :, columns(peer[3])]
                    remote(piece, piece, send_far.at[a, k], recv_far.at[a, k], me, q).wait_recv()

    def forward(g):
        low, high = groups[g]
        count = high - low
        size = count * block_rows
        here = slice(low * block_rows, high * block_rows)
        got = rows[1, low:high].reshape(size, model_width)
        gate_pre = jnp.dot(got, w_gate[...], preferred_element_type=jnp.float32)
        up_pre = jnp.dot(got, w_up[...], preferred_element_type=jnp.float32)
        sigmoid_gate = jax.nn.sigmoid(gate_pre)
        silu_gate = gate_pre * sigmoid_gate
        hidden[here, :] = (silu_gate * up_pre).astype(hidden.dtype)
        got = rows[0, low:high].reshape(size, model_width)
        hidden_grad = dot(got, w_down[...], 1, 1)
        gate_rows = (
            hidden_grad * up_pre * sigmoid_gate * (1.0 + gate_pre * (1.0 - sigmoid_gate))
        ).astype(jnp.bfloat16)
        up_rows = (hidden_grad * silu_gate).astype(jnp.bfloat16)
        gate_grad[here, :] = gate_rows
        up_grad[here, :] = up_rows
        for m in list(range(tp_count - 1, 0, -1)) + [0]:
            theirs = columns(peer[m])
            partial = dot(gate_rows, w_gate[theirs, :], 1, 1) + dot(up_rows, w_up[theirs, :], 1, 1)
            partial = partial.reshape(count, block_rows, width)
            if m == 0:
                own_part[low:high] = partial
            else:
                part[m - 1, low:high] = partial.astype(part.dtype)
                send(
                    remote(
                        part.at[m - 1, pl.ds(low, count)],
                        summed_in.at[m - 1, pl.ds(low, count)],
                        send_rs.at[g, m - 1],
                        recv_rs.at[g, m - 1],
                        me,
                        peer[m],
                    )
                )

    def give_back(g):
        low, high = groups[g]
        count = high - low
        total = own_part[low:high]
        for m in range(1, tp_count):
            piece = summed_in.at[m - 1, pl.ds(low, count)]
            remote(piece, piece, send_rs.at[g, m - 1], recv_rs.at[g, m - 1], me, q).wait_recv()
            total = total + summed_in[m - 1, low:high].astype(jnp.float32)
        total = total.astype(outgoing.dtype)
        for k in range(low, high):
            if k == 0:
                returned[0] = total[0]
            else:
                outgoing[k] = total[k - low]
                send(
                    remote(
                        outgoing.at[k], returned.at[k], send_back.at[k], recv_back.at[k], at[k], q
                    )
                )

    all_rows = sp_count * block_rows

    def down_grads():
        got = rows[0].reshape(all_rows, model_width)
        for m in range(tp_count):
            cut = slice(m * width, (m + 1) * width)
            grad_down[:, cut] = dot(hidden[...], got[:, cut], 0, 0).astype(grad_down.dtype)

    def input_grads(grads, out):
        for m in range(tp_count):
            cut = slice(m * width, (m + 1) * width)
            got = rows[1, :, :, cut].reshape(all_rows, width)
            out[cut, :] = dot(got, grads[...], 0, 0).astype(out.dtype)

    count = len(groups)
    with jax.named_scope("land#g=0"):
        land(0)
        land(1)
        relay(0)
    with jax.named_scope("weights"):
        for load in loads[2:5]:
            load.wait()
    with jax.named_scope("settle#g=0"):
        settle(0)
    with jax.named_scope("forward#g=0"):
        forward(0)
    for g in range(1, count):
        with jax.named_scope(f"relay#g={g}"):
            relay(g)
        if g + 1 < count:
            with jax.named_scope(f"land#g={g + 1}"):
                land(g + 1)
        elif g >= 2:
            with jax.named_scope("give#g=0"):
                give_back(0)
        with jax.named_scope(f"settle#g={g}"):
            settle(g)
        with jax.named_scope(f"forward#g={g}"):
            forward(g)
    for g in range(0 if count <= 2 else 1, count - 1):
        with jax.named_scope(f"give#g={g}"):
            give_back(g)
    with jax.named_scope("grad_down"):
        down_grads()
    with jax.named_scope(f"give#g={count - 1}"):
        give_back(count - 1)
    with jax.named_scope("grad_gate"):
        input_grads(gate_grad, grad_gate)
    with jax.named_scope("carry"):
        score_stage()
        carry_stage()
    with jax.named_scope("back"):
        for k in range(1, sp_count):
            remote(
                outgoing.at[k], returned.at[k], send_back.at[k], recv_back.at[k], me, q
            ).wait_recv()
    with jax.named_scope("combine"):
        total = dot(either[...], returned[...].reshape(all_rows, width), 0, 0)
        resid[:, mine] = (cot[:, mine].astype(jnp.float32) + total).astype(resid.dtype)
        piece = resid.at[:, mine]
        for m in range(tp_count - 1, 0, -1):
            send(remote(piece, piece, send_ag.at[m - 1], recv_ag.at[m - 1], me, peer[m]))

    core = lax.rem(me, 2)
    chip_rows = 2 * proj.shape[2]
    chips_here = width // chip_rows

    def project(m):
        piece = resid[:, columns(peer[m])]
        weights = w_proj[columns(peer[m]), :]
        part_here = dot(piece, mixer[...], 0, 0)
        chips = pl.ds(peer[m] * chips_here, chips_here)
        proj[chips] = part_here.reshape((chips_here,) + proj.shape[1:])
        send(
            remote(
                proj.at[chips, 1 - core],
                pair_in.at[chips],
                send_pair.at[m],
                recv_pair.at[m],
                at[1],
                q,
            )
        )
        return dot(weights, piece, 0, 1)

    with jax.named_scope("project#m=0"):
        loads[5].wait()
        out_grad = project(0)
    with jax.named_scope("grad_up"):
        input_grads(up_grad, grad_up)
    for m in range(1, tp_count):
        with jax.named_scope(f"gather#m={m}"):
            piece = resid.at[:, columns(peer[m])]
            remote(piece, piece, send_ag.at[m - 1], recv_ag.at[m - 1], me, q).wait_recv()
        with jax.named_scope(f"project#m={m}"):
            out_grad = out_grad + project(m)
    with jax.named_scope("query_states"):
        for h in range(heads):
            query = queries[key_part(h), :].astype(jnp.float32)
            for side in range(2):
                seen = exact_dot(query * reaches[reach_part(h, side), :], out_grad[value_part(h)], 1, 1)
                query_out[side, key_part(h), :] = seen.astype(query_out.dtype)
        for k in reversed(range(1, sp_count)):
            send(
                remote(
                    query_out.at[state_side(me, at[k], sp_count)],
                    query_all.at[me],
                    send_query.at[k],
                    recv_query.at[k],
                    at[k],
                    q,
                )
            )
    with jax.named_scope("pair"):
        for m in range(tp_count):
            chips = pl.ds(peer[m] * chips_here, chips_here)
            remote(
                proj.at[chips, 1 - core], pair_in.at[chips], send_pair.at[m], recv_pair.at[m], me, q
            ).wait_recv()
        for k in reversed(range(2, sp_count, 2)):
            chip = at[k] // 2
            proj_out[k // 2] = (proj[chip, core] + pair_in[chip]).astype(proj_out.dtype)
            send(
                remote(
                    proj_out.at[k // 2],
                    proj_in.at[k // 2],
                    send_proj.at[k // 2],
                    recv_proj.at[k // 2],
                    at[k],
                    q,
                )
            )
        chip = me // 2
        proj_total = proj[chip, core] + pair_in[chip]
    with jax.named_scope("retention"):
        for h in range(heads):
            query = queries[key_part(h), :].astype(jnp.float32)
            key = keys[key_part(h), :].astype(jnp.float32)
            value = values[value_part(h), :].astype(jnp.float32)
            grad = out_grad[value_part(h)]
            score_grad = mixing[h] * exact_dot(grad, value, 0, 0)
            to_end = score_scale * reaches[reach_part(h, 0), :]
            from_start = score_scale * reaches[reach_part(h, 1), :]
            out_reach = jnp.concatenate([grad * from_start, grad * to_end], axis=0)
            grad_queries[key_part(h), :] = exact_dot(key, score_grad, 1, 1) + exact_dot(
                key_carried[h], out_reach, 1, 0
            )
            grad_keys[key_part(h), :] = exact_dot(query, score_grad, 1, 0)
            grad_values[value_part(h), :] = exact_dot(grad, scores[h], 1, 0)
    with jax.named_scope("query_wait"):
        for k in range(1, sp_count):
            piece = query_all.at[at[k]]
            remote(piece, piece, send_query.at[k], recv_query.at[k], me, q).wait_recv()
    with jax.named_scope("finish"):
        for h in range(heads):
            key = keys[key_part(h), :].astype(jnp.float32)
            value = values[value_part(h), :].astype(jnp.float32)
            to_end = score_scale * reaches[reach_part(h, 0), :]
            from_start = score_scale * reaches[reach_part(h, 1), :]
            carried = []
            for decay in decays(h):
                total = jnp.zeros((key_size, value_size), jnp.float32)
                for b in range(sp_count):
                    total = total + decay[b] * query_all[b, key_part(h), :].astype(jnp.float32)
                carried.append(total)
            value_reach = jnp.concatenate([value * from_start, value * to_end], axis=0)
            key_reach = jnp.concatenate([key * from_start, key * to_end], axis=0)
            grad_keys[key_part(h), :] = grad_keys[key_part(h), :] + exact_dot(
                jnp.concatenate(carried, axis=1), value_reach, 1, 0
            )
            grad_values[value_part(h), :] = grad_values[value_part(h), :] + exact_dot(
                jnp.concatenate(carried, axis=0), key_reach, 0, 0
            )
    with jax.named_scope("proj_wait"):
        for i in range(1, sp_count // 2):
            remote(
                proj_out.at[i], proj_in.at[i], send_proj.at[i], recv_proj.at[i], me, q
            ).wait_recv()
            proj_total = proj_total + proj_in[i].astype(jnp.float32)
        grad_proj[...] = proj_total
    for copy in waits:
        copy.wait_send()


def experts(
    ids, group, weight, rates, queries, keys, values, mixer, cot, inp, gate, up, down, proj, capacity, sp_count, tp_count
):
    tokens, model_width = cot.shape
    width = model_width // tp_count
    hidden_width = gate.shape[2]
    heads, length = rates.shape
    state_rows = keys.shape[0] + 8 * heads
    key_size = keys.shape[0] // heads
    value_size = values.shape[0] // heads
    head_columns = mixer.shape[1]
    proj_rows = model_width // sp_count
    block_rows = -(-capacity // 16) * 16
    all_rows = sp_count * block_rows
    chips = sp_count // 2
    quarter = sp_count // 4
    groups = [(i * quarter, (i + 1) * quarter) for i in range(4)]
    kind = cot.dtype
    full = jnp.float32
    dma = pltpu.SemaphoreType.DMA
    vmem = pltpu.VMEM
    return pl.pallas_call(
        functools.partial(experts_kernel, sp_count, tp_count, groups),
        out_shape=(
            vmem((model_width, hidden_width), kind),
            vmem((model_width, hidden_width), kind),
            vmem((hidden_width, model_width), kind),
            vmem((proj_rows, head_columns), full),
            vmem(queries.shape, full),
            vmem(keys.shape, full),
            vmem(values.shape, full),
        ),
        in_specs=[VMEM] * 8 + [ANY] * 6,
        out_specs=(VMEM,) * 7,
        scratch_shapes=[
            vmem((tokens, model_width), kind),
            vmem((tokens, model_width), kind),
            vmem((model_width, hidden_width), kind),
            vmem((model_width, hidden_width), kind),
            vmem((hidden_width, model_width), kind),
            vmem(proj.shape, kind),
            vmem((all_rows, ids.shape[0] * tokens), jnp.bfloat16),
            vmem((all_rows, tokens), jnp.bfloat16),
            vmem((ids.shape[0] * tokens, model_width), kind),
            vmem((sp_count, 2, block_rows, width), kind),
            vmem((2, block_rows, model_width), kind),
            vmem((2, sp_count, block_rows, model_width), kind),
            vmem((2, state_rows, value_size), full),
            vmem((sp_count, state_rows, value_size), full),
            vmem((tokens, model_width), kind),
            vmem((heads, length, length), full),
            vmem((heads, length, length), full),
            vmem((8 * heads, length), full),
            vmem((heads, key_size, 2 * value_size), full),
            vmem((chips, 2, proj_rows, head_columns), full),
            vmem((chips, proj_rows, head_columns), full),
            vmem((chips, proj_rows, head_columns), kind),
            vmem((chips, proj_rows, head_columns), kind),
            vmem((2, keys.shape[0], value_size), kind),
            vmem((sp_count, keys.shape[0], value_size), kind),
            vmem((all_rows, hidden_width), kind),
            vmem((all_rows, hidden_width), kind),
            vmem((all_rows, hidden_width), kind),
            vmem((tp_count - 1, sp_count, block_rows, width), kind),
            vmem((sp_count, block_rows, width), full),
            vmem((tp_count - 1, sp_count, block_rows, width), kind),
            vmem((sp_count, block_rows, width), kind),
            vmem((sp_count, block_rows, width), kind),
            dma((6,)),
            dma((sp_count,)),
            dma((sp_count,)),
            dma((sp_count, tp_count - 1)),
            dma((sp_count, tp_count - 1)),
            dma((2, sp_count)),
            dma((2, sp_count)),
            dma((sp_count,)),
            dma((sp_count,)),
            dma((len(groups), tp_count - 1)),
            dma((len(groups), tp_count - 1)),
            dma((sp_count,)),
            dma((sp_count,)),
            dma((tp_count - 1,)),
            dma((tp_count - 1,)),
            dma((tp_count,)),
            dma((tp_count,)),
            dma((chips,)),
            dma((chips,)),
            dma((sp_count,)),
            dma((sp_count,)),
        ],
        compiler_params=pltpu.CompilerParams(
            collective_id=0, has_side_effects=True, vmem_limit_bytes=48 * 1024 * 1024
        ),
    )(ids, group, weight, rates, queries, keys, values, mixer, cot, inp, gate, up, down, proj)


def on_device(
    cotangent,
    moe_input,
    expert_ids,
    group_weight,
    expert_weight,
    mixer_out,
    queries,
    key_vectors,
    value_vectors,
    decay_rates,
    proj_weight,
    gate_weight,
    up_weight,
    down_weight,
):
    sp_count = lax.axis_size("sp")
    tp_count = lax.axis_size("tp")
    experts_all = gate_weight.shape[0] * sp_count
    rows_here = cotangent.shape[0]
    top_count = expert_ids.shape[1]
    capacity = 3 * top_count * rows_here // (2 * experts_all)
    grad_gate, grad_up, grad_down, grad_proj, grad_queries, grad_keys, grad_values = experts(
        expert_ids.T,
        group_weight[None, :],
        expert_weight.T,
        decay_rates,
        queries,
        key_vectors,
        value_vectors,
        mixer_out,
        cotangent,
        moe_input,
        gate_weight,
        up_weight,
        down_weight,
        proj_weight,
        capacity,
        sp_count,
        tp_count,
    )
    return (
        grad_gate[None],
        grad_up[None],
        grad_down[None],
        grad_proj,
        grad_queries,
        grad_keys,
        grad_values,
    )


def solution(mesh):
    return jax.shard_map(
        on_device,
        mesh=mesh,
        in_specs=(
            P("sp", None),
            P("sp", None),
            P("sp", None),
            P("sp"),
            P("sp", None),
            P("sp", "tp"),
            P("tp", "sp"),
            P("tp", "sp"),
            P("tp", "sp"),
            P("tp", "sp"),
            P(None, "tp"),
            P("sp", None, "tp"),
            P("sp", None, "tp"),
            P("sp", "tp", None),
        ),
        out_specs=(
            P("sp", None, "tp"),
            P("sp", None, "tp"),
            P("sp", "tp", None),
            P("sp", "tp"),
            P("tp", "sp"),
            P("tp", "sp"),
            P("tp", "sp"),
        ),
        check_vma=False,
    )
```

```python
import functools

import jax
import jax.numpy as jnp
from jax import lax
from jax.experimental import pallas as pl
from jax.experimental.pallas import tpu as pltpu
from jax.sharding import PartitionSpec as P

MESH = pl.DeviceIdType.MESH
VMEM = pl.BlockSpec(memory_space=pltpu.VMEM)
ANY = pl.BlockSpec(memory_space=pl.ANY)


def partner(place, k, count):
    if k == 0:
        return place
    out = 0
    bit = 1
    while bit < count:
        b = lax.rem(place // bit, 2)
        out = out + bit * ((1 - b) if k & bit else b)
        bit *= 2
    return out


def remote(src, dst, send_sem, recv_sem, sp_place, tp_place):
    return pltpu.make_async_remote_copy(
        src_ref=src,
        dst_ref=dst,
        send_sem=send_sem,
        recv_sem=recv_sem,
        device_id={"sp": sp_place, "tp": tp_place},
        device_id_type=MESH,
    )


def state_side(here, there, count):
    return (here + count - there) // count


def dot(a, b, a_dim, b_dim):
    return lax.dot_general(
        a, b, (((a_dim,), (b_dim,)), ((), ())), preferred_element_type=jnp.float32
    )


def experts_kernel(
    sp_count, tp_count, order, groups,
    ids_hbm, group_hbm, weight_hbm, rates_hbm, queries_hbm, keys_hbm, values_hbm, mixer_hbm,
    cot_hbm, inp_hbm, gate_hbm, up_hbm, down_hbm, proj_hbm,
    grad_gate, grad_up, grad_down, grad_proj, grad_queries, grad_keys, grad_values,
    ids, group, weight, rates, queries, keys, values, mixer, cot, inp, w_gate, w_up, w_down, w_proj, picks, either, scaled, z_src, pair_src, rows, state, state_all, resid,
    scores, mixing, reaches, key_carried, proj, pair_in, proj_out, proj_in, query_out, query_all,
    hidden, gate_grad, up_grad, part, own_part, kept, summed_in, outgoing, returned,
    load_sem, send_sem, recv_z, recv_xy, recv_far, recv_rs, recv_hop, recv_ag, recv_all,
):
    me = lax.axis_index("sp")
    q = lax.axis_index("tp")
    tokens, model_width = cot.shape
    width = model_width // tp_count
    block_rows = rows.shape[2]
    hidden_width = w_gate.shape[1]
    square = tp_count == 4
    at = [partner(me, k, sp_count) for k in order]
    peer = [partner(q, m, tp_count) for m in range(tp_count)]

    def columns(place):
        return pl.ds(pl.multiple_of(place * width, width), width)

    mine = columns(q)
    halves = 2 if width == 2 * proj.shape[2] and proj.shape[2] % 128 == 0 else 1

    def half_columns(place, j):
        size = width // halves
        return pl.ds(pl.multiple_of(place * width + j * size, size), size)

    loads = []
    for i, (src, dst) in enumerate(
        (
            (ids_hbm, ids),
            (group_hbm, group),
            (weight_hbm, weight),
            (cot_hbm, cot),
            (inp_hbm, inp),
            (rates_hbm, rates),
            (keys_hbm, keys),
            (values_hbm, values),
            (gate_hbm.at[0], w_gate),
            (up_hbm.at[0], w_up),
            (down_hbm.at[0], w_down),
            (queries_hbm, queries),
            (mixer_hbm, mixer),
            (proj_hbm, w_proj),
        )
    ):
        copy = pltpu.make_async_copy(src, dst, load_sem.at[i])
        copy.start()
        loads.append(copy)

    barrier = pltpu.get_barrier_semaphore()
    for k in range(1, sp_count):
        pl.semaphore_signal(
            barrier, inc=1, device_id={"sp": at[k], "tp": q}, device_id_type=MESH
        )
    for m in range(1, tp_count):
        pl.semaphore_signal(
            barrier, inc=1, device_id={"sp": me, "tp": peer[m]}, device_id_type=MESH
        )

    with jax.named_scope("slots"):
        for load in loads[:3]:
            load.wait()
        top_count = ids.shape[0]
        expert = lax.broadcasted_iota(jnp.int32, (sp_count, tokens), 0)
        named = [(ids[j : j + 1, :] == expert).astype(jnp.float32) for j in range(top_count)]
        earlier = lax.broadcasted_iota(jnp.int32, (tokens, tokens), 0) < lax.broadcasted_iota(
            jnp.int32, (tokens, tokens), 1
        )
        before = jnp.dot(
            sum(named).astype(jnp.bfloat16),
            earlier.astype(jnp.float32).astype(jnp.bfloat16),
            preferred_element_type=jnp.float32,
        )
        slots = []
        route = jnp.zeros((8, tokens), jnp.float32)
        lane_of = lax.broadcasted_iota(jnp.int32, (8, tokens), 0)
        for j in range(top_count):
            rank = jnp.sum(named[j] * before, axis=0, keepdims=True).astype(jnp.int32)
            before = before + named[j]
            slots.append(ids[j : j + 1, :] * block_rows + rank)
            route = jnp.where(lane_of == j, group[...] * weight[j : j + 1, :], route)
        route = jnp.transpose(route)
        row_of = lax.broadcasted_iota(jnp.int32, (block_rows, tokens), 0)
        for k in range(sp_count):
            here = pl.ds(k * block_rows, block_rows)
            pick = [(s == row_of + at[k] * block_rows).astype(jnp.float32) for s in slots]
            for j in range(top_count):
                picks[here, j * tokens : (j + 1) * tokens] = pick[j].astype(jnp.bfloat16)
            either[here, :] = sum(pick).astype(jnp.bfloat16)

    with jax.named_scope("pack"):
        loads[3].wait()
        loads[4].wait()
        cot_mine = cot[:, mine].astype(jnp.float32)
        scaled_mine = jnp.concatenate(
            [(cot_mine * route[:, j : j + 1]).astype(jnp.bfloat16) for j in range(top_count)], axis=0
        )
        first = 2 * block_rows
        cot_out = jnp.dot(picks[first:, :], scaled_mine, preferred_element_type=jnp.float32)
        inp_out = jnp.dot(either[first:, :], inp[:, mine], preferred_element_type=jnp.float32)
        for k in range(2, sp_count):
            here = slice((k - 2) * block_rows, (k - 1) * block_rows)
            z_src[k, 0] = cot_out[here].astype(z_src.dtype)
            z_src[k, 1] = inp_out[here].astype(z_src.dtype)
    with jax.named_scope("barrier"):
        pl.semaphore_wait(barrier, sp_count - 1 + tp_count - 1)

    pending = []

    def start(copy):
        copy.start()

    for k in range(2, sp_count):
        start(remote(z_src.at[k], rows.at[:, k, :, mine], send_sem.at[0], recv_z.at[k], at[k], q))
    with jax.named_scope("near"):
        cot_all = cot[...].astype(jnp.float32)
        for j in range(top_count):
            scaled[j * tokens : (j + 1) * tokens, :] = (cot_all * route[:, j : j + 1]).astype(scaled.dtype)
        cot_out = jnp.dot(picks[:first, :], scaled[...], preferred_element_type=jnp.float32)
        inp_out = jnp.dot(either[:first, :], inp[...], preferred_element_type=jnp.float32)
        pair_src[0] = cot_out[block_rows:].astype(pair_src.dtype)
        pair_src[1] = inp_out[block_rows:].astype(pair_src.dtype)
        start(remote(pair_src, rows.at[:, 1], send_sem.at[1], recv_z.at[1], at[1], q))
        rows[0, 0] = cot_out[:block_rows].astype(rows.dtype)
        rows[1, 0] = inp_out[:block_rows].astype(rows.dtype)

    exact = lax.Precision.HIGHEST
    heads, length = rates.shape
    key_size = keys.shape[0] // heads
    value_size = values.shape[0] // heads
    score_scale = key_size ** (-0.5)

    def exact_dot(a, b, a_dim, b_dim):
        return lax.dot_general(
            a,
            b,
            (((a_dim,), (b_dim,)), ((), ())),
            precision=exact,
            preferred_element_type=jnp.float32,
        )

    def key_part(h):
        return slice(h * key_size, (h + 1) * key_size)

    def value_part(h):
        return slice(h * value_size, (h + 1) * value_size)

    def reach_part(h, side):
        return slice(8 * h + side, 8 * h + side + 1)

    with jax.named_scope("states"):
        for load in loads[5:8]:
            load.wait()
        upto = lax.broadcasted_iota(jnp.int32, (length, length), 0) <= lax.broadcasted_iota(
            jnp.int32, (length, length), 1
        )
        for h in range(heads):
            rate = jnp.broadcast_to(rates[h : h + 1, :], (8, length))
            prefixes = exact_dot(rate, upto.astype(jnp.float32), 1, 0)
            prefix = prefixes[0:1]
            ending = prefix[:, length - 1 : length]
            gap = jnp.transpose(prefixes)[:, 0:1] - prefix
            mixing[h] = score_scale * jnp.exp(-jnp.abs(gap))
            key = keys[key_part(h), :].astype(jnp.float32)
            value = values[value_part(h), :].astype(jnp.float32)
            top = h * (key_size + 8)
            for side, reach in enumerate((jnp.exp(prefix - ending), jnp.exp(-prefix))):
                reaches[reach_part(h, side), :] = reach
                state[side, top : top + key_size, :] = exact_dot(key * reach, value, 1, 1)
                state[side, top + key_size : top + key_size + 8, :] = jnp.broadcast_to(
                    ending, (8, value_size)
                )
        state_all[me] = state[0]
        query_all[me] = jnp.zeros(query_all.shape[1:], query_all.dtype)
        for k in range(1, sp_count):
            start(
                remote(
                    state.at[state_side(me, at[k], sp_count)],
                    state_all.at[me],
                    send_sem.at[4],
                    recv_all.at[0],
                    at[k],
                    q,
                )
            )

    def score_stage():
        loads[11].wait()
        for h in range(heads):
            query = queries[key_part(h), :].astype(jnp.float32)
            key = keys[key_part(h), :].astype(jnp.float32)
            scores[h] = mixing[h] * exact_dot(query, key, 0, 0)

    def decays(h):
        total_at = h * (key_size + 8) + key_size
        low, high = [None] * sp_count, [None] * sp_count
        totals = [state_all[b, total_at : total_at + 1, :] for b in range(sp_count)]
        run = jnp.zeros((1, value_size), jnp.float32)
        for b in reversed(range(sp_count)):
            low[b] = jnp.where(b < me, jnp.exp(-run), 0.0)
            run = run + jnp.where(b < me, totals[b], 0.0)
        run = jnp.zeros((1, value_size), jnp.float32)
        for b in range(sp_count):
            high[b] = jnp.where(b > me, jnp.exp(-run), 0.0)
            run = run + jnp.where(b > me, totals[b], 0.0)
        return low, high

    def carry_stage():
        piece = state_all.at[pl.ds(0, sp_count - 1)]
        remote(piece, piece, send_sem.at[4], recv_all.at[0], me, q).wait_recv()
        for h in range(heads):
            top = h * (key_size + 8)
            for side, decay in enumerate(decays(h)):
                total = jnp.zeros((key_size, value_size), jnp.float32)
                for b in range(sp_count):
                    total = total + decay[b] * state_all[b, top : top + key_size, :]
                key_carried[h, :, side * value_size : (side + 1) * value_size] = total

    def land(g):
        for k in range(*groups[g]):
            if k < 2:
                continue
            piece = rows.at[:, k, :, mine]
            remote(z_src.at[k], piece, send_sem.at[0], recv_z.at[k], me, q).wait_recv()
            for m in range(1, tp_count):
                if square and m == 3:
                    continue
                start(
                    remote(piece, piece, send_sem.at[2], recv_xy.at[k - 2, m - 1], me, peer[m])
                )

    def relay(g):
        for k in range(*groups[g]):
            if k < 2:
                continue
            for m in range(1, tp_count):
                if square and m == 3:
                    continue
                piece = rows.at[:, k, :, columns(peer[m])]
                remote(piece, piece, send_sem.at[2], recv_xy.at[k - 2, m - 1], me, q).wait_recv()
                if square:
                    a = m - 1
                    half = rows.at[a, k, :, columns(peer[m])]
                    start(
                        remote(half, half, send_sem.at[3], recv_far.at[a, k - 2], me, peer[3 - m])
                    )

    def settle(g):
        for k in range(*groups[g]):
            if k == 1:
                remote(pair_src, rows.at[:, 1], send_sem.at[1], recv_z.at[1], me, q).wait_recv()
            if k >= 2 and square:
                for a in range(2):
                    piece = rows.at[a, k, :, columns(peer[3])]
                    remote(piece, piece, send_sem.at[3], recv_far.at[a, k - 2], me, q).wait_recv()

    def forward(g):
        low, high = groups[g]
        count = high - low
        size = count * block_rows
        here = slice(low * block_rows, high * block_rows)
        got = rows[1, low:high].reshape(size, model_width)
        gate_pre = jnp.dot(got, w_gate[...], preferred_element_type=jnp.float32)
        up_pre = jnp.dot(got, w_up[...], preferred_element_type=jnp.float32)
        sigmoid_gate = jax.nn.sigmoid(gate_pre)
        silu_gate = gate_pre * sigmoid_gate
        hidden[here, :] = (silu_gate * up_pre).astype(hidden.dtype)
        got = rows[0, low:high].reshape(size, model_width)
        hidden_grad = dot(got, w_down[...], 1, 1)
        gate_rows = (
            hidden_grad * up_pre * sigmoid_gate * (1.0 + gate_pre * (1.0 - sigmoid_gate))
        ).astype(jnp.bfloat16)
        up_rows = (hidden_grad * silu_gate).astype(jnp.bfloat16)
        gate_grad[here, :] = gate_rows
        up_grad[here, :] = up_rows

        def partial(m):
            theirs = columns(peer[m])
            total = dot(gate_rows, w_gate[theirs, :], 1, 1) + dot(up_rows, w_up[theirs, :], 1, 1)
            return total.reshape(count, block_rows, width)

        if square:
            half = count // 2
            middle = low + half
            total = partial(3).astype(part.dtype)
            part[1, low:high] = total
            total = partial(1)
            part[0, low:middle] = total[:half].astype(part.dtype)
            kept[middle:high] = total[half:]
            pending.append(first_hop(g, 0))
            total = partial(2)
            part[0, middle:high] = total[half:].astype(part.dtype)
            kept[low:middle] = total[:half]
            pending.append(first_hop(g, 1))
        else:
            for m in range(tp_count - 1, 0, -1):
                part[m - 1, low:high] = partial(m).astype(part.dtype)
                piece = pl.ds(low, count)
                start(
                    remote(
                        part.at[m - 1, piece],
                        summed_in.at[m - 1, piece],
                        send_sem.at[5],
                        recv_rs.at[g, m - 1],
                        me,
                        peer[m],
                    )
                )
        own_part[low:high] = partial(0)

    def flush():
        while pending:
            start(pending.pop(0))

    def hop_blocks(g, side):
        low, high = groups[g]
        half = (high - low) // 2
        return (low, low + half) if side == 0 else (low + half, high)

    def first_hop(g, side):
        low, high = hop_blocks(g, side)
        piece = pl.ds(low, high - low)
        return remote(
            part.at[pl.ds(0, 2), piece],
            summed_in.at[pl.ds(0, 2), piece],
            send_sem.at[5],
            recv_rs.at[g, side],
            me,
            peer[1 + side],
        )

    def second_hop(g, side):
        low, high = hop_blocks(g, side)
        piece = pl.ds(low, high - low)
        return remote(
            part.at[2, piece],
            summed_in.at[2, piece],
            send_sem.at[6],
            recv_hop.at[g, side],
            me,
            peer[2 - side],
        )

    def hop(g):
        if not square:
            return
        for side in range(2):
            low, high = hop_blocks(g, side)
            first_hop(g, side).wait_recv()
            total = kept[low:high] + summed_in[1, low:high].astype(jnp.float32)
            part[2, low:high] = total.astype(part.dtype)
            start(second_hop(g, side))

    def give_back(g):
        low, high = groups[g]
        count = high - low
        total = own_part[low:high]
        if square:
            for side in range(2):
                second_hop(g, side).wait_recv()
            total = total + summed_in[0, low:high].astype(jnp.float32)
            total = total + summed_in[2, low:high].astype(jnp.float32)
        else:
            for m in range(1, tp_count):
                piece = summed_in.at[m - 1, pl.ds(low, count)]
                remote(piece, piece, send_sem.at[5], recv_rs.at[g, m - 1], me, q).wait_recv()
                total = total + summed_in[m - 1, low:high].astype(jnp.float32)
        total = total.astype(outgoing.dtype)
        for k in range(low, high):
            if k == 0:
                returned[0] = total[0]
            else:
                outgoing[k] = total[k - low]
                start(
                    remote(
                        outgoing.at[k], returned.at[k], send_sem.at[7], recv_all.at[1], at[k], q
                    )
                )

    all_rows = sp_count * block_rows

    def down_grads():
        got = rows[0].reshape(all_rows, model_width)
        for m in range(tp_count):
            cut = slice(m * width, (m + 1) * width)
            grad_down[:, cut] = dot(hidden[...], got[:, cut], 0, 0).astype(grad_down.dtype)

    def input_grads(grads, out):
        for m in range(tp_count):
            cut = slice(m * width, (m + 1) * width)
            got = rows[1, :, :, cut].reshape(all_rows, width)
            out[cut, :] = dot(got, grads[...], 0, 0).astype(out.dtype)

    count = len(groups)
    with jax.named_scope("weights"):
        for load in loads[8:11]:
            load.wait()
    with jax.named_scope("land#g=0"):
        land(0)
        relay(0)
        settle(0)
    with jax.named_scope("forward#g=0"):
        forward(0)
    flush()
    with jax.named_scope("land#g=1"):
        land(1)
    with jax.named_scope("hop#g=0"):
        hop(0)
    with jax.named_scope("relay#g=1"):
        relay(1)
    with jax.named_scope("land#g=2"):
        land(2)
    with jax.named_scope("settle#g=1"):
        settle(1)
    with jax.named_scope("forward#g=1"):
        forward(1)
    with jax.named_scope("relay#g=2"):
        relay(2)
    flush()
    with jax.named_scope("land#g=3"):
        land(3)
    with jax.named_scope("settle#g=2"):
        settle(2)
    with jax.named_scope("forward#g=2"):
        forward(2)
    flush()
    with jax.named_scope("relay#g=3"):
        relay(3)
    with jax.named_scope("hop#g=1"):
        hop(1)
    with jax.named_scope("give#g=0"):
        give_back(0)
    with jax.named_scope("hop#g=2"):
        hop(2)
    with jax.named_scope("settle#g=3"):
        settle(3)
    with jax.named_scope("forward#g=3"):
        forward(3)
    flush()
    with jax.named_scope("give#g=1"):
        give_back(1)
    with jax.named_scope("give#g=2"):
        give_back(2)
    with jax.named_scope("grad_down"):
        down_grads()
    with jax.named_scope("hop#g=3"):
        hop(3)
    with jax.named_scope("grad_gate"):
        input_grads(gate_grad, grad_gate)
    with jax.named_scope("give#g=3"):
        give_back(3)
    with jax.named_scope("carry"):
        score_stage()
        carry_stage()
    with jax.named_scope("back"):
        piece = returned.at[pl.ds(0, sp_count - 1)]
        remote(piece, piece, send_sem.at[7], recv_all.at[1], me, q).wait_recv()
    with jax.named_scope("combine"):
        total = dot(either[...], returned[...].reshape(all_rows, width), 0, 0)
        resid[:, mine] = (cot[:, mine].astype(jnp.float32) + total).astype(resid.dtype)
        for j in range(halves):
            piece = resid.at[:, half_columns(q, j)]
            for m in range(tp_count - 1, 0, -1):
                start(remote(piece, piece, send_sem.at[8], recv_ag.at[m - 1, j], me, peer[m]))

    core = lax.rem(me, 2)
    chips_here = width // (2 * proj.shape[2])

    def project(m, j):
        piece = resid[:, half_columns(peer[m], j)]
        part_here = dot(piece, mixer[...], 0, 0)
        chips = pl.ds(peer[m] * chips_here, chips_here)
        if halves == 2:
            proj[chips, j] = part_here.reshape((chips_here,) + proj.shape[2:])
        else:
            proj[chips] = part_here.reshape((chips_here,) + proj.shape[1:])
        return dot(w_proj[half_columns(peer[m], j), :], piece, 0, 1)

    def pair_copy():
        return remote(
            proj.at[:, 1 - core], pair_in, send_sem.at[9], recv_all.at[2], at[1], q
        )

    def pair_total(chip):
        return proj[chip, core] + pair_in[chip]

    def across_chips():
        pair_copy().wait_recv()
        for k in reversed(range(2, sp_count, 2)):
            proj_out[k // 2] = pair_total(at[k] // 2).astype(proj_out.dtype)
            start(
                remote(
                    proj_out.at[k // 2],
                    proj_in.at[k // 2],
                    send_sem.at[10],
                    recv_all.at[3],
                    at[k],
                    q,
                )
            )
        grad_proj[...] = pair_total(me // 2)

    with jax.named_scope("project#m=0"):
        loads[12].wait()
        loads[13].wait()
        out_grad = project(0, 0)
        for j in range(1, halves):
            out_grad = out_grad + project(0, j)
    with jax.named_scope("grad_up"):
        input_grads(up_grad, grad_up)
    for j in range(halves):
        for m in range(1, tp_count):
            with jax.named_scope(f"gather#m={m}#j={j}"):
                piece = resid.at[:, half_columns(peer[m], j)]
                remote(piece, piece, send_sem.at[8], recv_ag.at[m - 1, j], me, q).wait_recv()
            with jax.named_scope(f"project#m={m}#j={j}"):
                out_grad = out_grad + project(m, j)
        if halves == 2:
            with jax.named_scope(f"pair#j={j}"):

                @pl.when(core != j)
                def _():
                    pair_copy().start()

                if j == 0:

                    @pl.when(core == j)
                    def _():
                        across_chips()

    if halves == 1:
        pair_copy().start()
    with jax.named_scope("query_states"):
        for h in range(heads):
            query = queries[key_part(h), :].astype(jnp.float32)
            for side in range(2):
                seen = exact_dot(query * reaches[reach_part(h, side), :], out_grad[value_part(h)], 1, 1)
                query_out[side, key_part(h), :] = seen.astype(query_out.dtype)
        for k in reversed(range(1, sp_count)):
            start(
                remote(
                    query_out.at[state_side(me, at[k], sp_count)],
                    query_all.at[me],
                    send_sem.at[11],
                    recv_all.at[4],
                    at[k],
                    q,
                )
            )
    with jax.named_scope("pair"):
        if halves == 1:
            across_chips()
        else:

            @pl.when(core == 1)
            def _():
                across_chips()

    with jax.named_scope("retention"):
        for h in range(heads):
            query = queries[key_part(h), :].astype(jnp.float32)
            key = keys[key_part(h), :].astype(jnp.float32)
            value = values[value_part(h), :].astype(jnp.float32)
            grad = out_grad[value_part(h)]
            score_grad = mixing[h] * exact_dot(grad, value, 0, 0)
            to_end = score_scale * reaches[reach_part(h, 0), :]
            from_start = score_scale * reaches[reach_part(h, 1), :]
            out_reach = jnp.concatenate([grad * from_start, grad * to_end], axis=0)
            grad_queries[key_part(h), :] = exact_dot(key, score_grad, 1, 1) + exact_dot(
                key_carried[h], out_reach, 1, 0
            )
            grad_keys[key_part(h), :] = exact_dot(query, score_grad, 1, 0)
            grad_values[value_part(h), :] = exact_dot(grad, scores[h], 1, 0)
    with jax.named_scope("query_wait"):
        piece = query_all.at[pl.ds(0, sp_count - 1)]
        remote(piece, piece, send_sem.at[11], recv_all.at[4], me, q).wait_recv()
    with jax.named_scope("finish"):
        for h in range(heads):
            key = keys[key_part(h), :].astype(jnp.float32)
            value = values[value_part(h), :].astype(jnp.float32)
            to_end = score_scale * reaches[reach_part(h, 0), :]
            from_start = score_scale * reaches[reach_part(h, 1), :]
            carried = []
            for decay in decays(h):
                total = jnp.zeros((key_size, value_size), jnp.float32)
                for b in range(sp_count):
                    total = total + decay[b] * query_all[b, key_part(h), :].astype(jnp.float32)
                carried.append(total)
            value_reach = jnp.concatenate([value * from_start, value * to_end], axis=0)
            key_reach = jnp.concatenate([key * from_start, key * to_end], axis=0)
            grad_keys[key_part(h), :] = grad_keys[key_part(h), :] + exact_dot(
                jnp.concatenate(carried, axis=1), value_reach, 1, 0
            )
            grad_values[value_part(h), :] = grad_values[value_part(h), :] + exact_dot(
                jnp.concatenate(carried, axis=0), key_reach, 0, 0
            )
    with jax.named_scope("proj_wait"):
        piece = proj_in.at[pl.ds(1, sp_count // 2 - 1)]
        remote(piece, piece, send_sem.at[10], recv_all.at[3], me, q).wait_recv()
        proj_total = grad_proj[...]
        for i in range(1, sp_count // 2):
            proj_total = proj_total + proj_in[i].astype(jnp.float32)
        grad_proj[...] = proj_total
    with jax.named_scope("sent"):
        others = pl.ds(0, sp_count - 2)
        crossing = 2 if square else tp_count - 1
        sent = [
            rows.at[:, others, :, pl.ds(0, width)],
            pair_src,
            rows.at[:, others, :, pl.ds(0, crossing * width)],
            rows.at[:, others, :, pl.ds(0, width)] if square else None,
            state_all.at[pl.ds(0, sp_count - 1)],
            part.at[pl.ds(0, 2)] if square else part,
            part.at[2] if square else None,
            outgoing.at[pl.ds(0, sp_count - 1)],
            resid.at[:, pl.ds(0, (tp_count - 1) * width)],
            pair_in,
            proj_out.at[pl.ds(0, sp_count // 2 - 1)],
            query_all.at[pl.ds(0, sp_count - 1)],
        ]
        for i, piece in enumerate(sent):
            if piece is not None:
                remote(piece, piece, send_sem.at[i], recv_all.at[0], me, q).wait_send()


def store_kernel(*refs):
    count = (len(refs) - 1) // 2
    copies = [
        pltpu.make_async_copy(refs[i], refs[count + i], refs[-1].at[i]) for i in range(count)
    ]
    for copy in copies:
        copy.start()
    for copy in copies:
        copy.wait()


def store(arrays):
    return pl.pallas_call(
        store_kernel,
        out_shape=tuple(jax.ShapeDtypeStruct(a.shape, a.dtype) for a in arrays),
        in_specs=[VMEM] * len(arrays),
        out_specs=(ANY,) * len(arrays),
        scratch_shapes=[pltpu.SemaphoreType.DMA((len(arrays),))],
        compiler_params=pltpu.CompilerParams(vmem_limit_bytes=16 * 1024 * 1024),
    )(*arrays)


def experts(
    ids, group, weight, rates, queries, keys, values, mixer, cot, inp, gate, up, down, proj, capacity, sp_count, tp_count
):
    tokens, model_width = cot.shape
    width = model_width // tp_count
    hidden_width = gate.shape[2]
    heads, length = rates.shape
    state_rows = keys.shape[0] + 8 * heads
    key_size = keys.shape[0] // heads
    value_size = values.shape[0] // heads
    head_columns = mixer.shape[1]
    proj_rows = model_width // sp_count
    block_rows = -(-capacity // 16) * 16
    all_rows = sp_count * block_rows
    chips = sp_count // 2
    quarter = sp_count // 4
    pairs = [0, 1] + list(range(sp_count // 2 - 1, 1, -1))
    order = [k for pair in pairs for k in (2 * pair, 2 * pair + 1)]
    groups = [(i * quarter, (i + 1) * quarter) for i in range(4)]
    crossing = 2 if tp_count == 4 else tp_count - 1
    kind = cot.dtype
    full = jnp.float32
    dma = pltpu.SemaphoreType.DMA
    vmem = pltpu.VMEM
    return pl.pallas_call(
        functools.partial(experts_kernel, sp_count, tp_count, order, groups),
        out_shape=(
            vmem((model_width, hidden_width), kind),
            vmem((model_width, hidden_width), kind),
            vmem((hidden_width, model_width), kind),
            vmem((proj_rows, head_columns), full),
            vmem(queries.shape, full),
            vmem(keys.shape, full),
            vmem(values.shape, full),
        ),
        in_specs=[ANY] * 14,
        out_specs=(VMEM,) * 7,
        scratch_shapes=[
            vmem(ids.shape, ids.dtype),
            vmem(group.shape, group.dtype),
            vmem(weight.shape, weight.dtype),
            vmem(rates.shape, rates.dtype),
            vmem(queries.shape, queries.dtype),
            vmem(keys.shape, keys.dtype),
            vmem(values.shape, values.dtype),
            vmem(mixer.shape, mixer.dtype),
            vmem((tokens, model_width), kind),
            vmem((tokens, model_width), kind),
            vmem((model_width, hidden_width), kind),
            vmem((model_width, hidden_width), kind),
            vmem((hidden_width, model_width), kind),
            vmem(proj.shape, kind),
            vmem((all_rows, ids.shape[0] * tokens), jnp.bfloat16),
            vmem((all_rows, tokens), jnp.bfloat16),
            vmem((ids.shape[0] * tokens, model_width), kind),
            vmem((sp_count, 2, block_rows, width), kind),
            vmem((2, block_rows, model_width), kind),
            vmem((2, sp_count, block_rows, model_width), kind),
            vmem((2, state_rows, value_size), full),
            vmem((sp_count, state_rows, value_size), full),
            vmem((tokens, model_width), kind),
            vmem((heads, length, length), full),
            vmem((heads, length, length), full),
            vmem((8 * heads, length), full),
            vmem((heads, key_size, 2 * value_size), full),
            vmem((chips, 2, proj_rows, head_columns), full),
            vmem((chips, proj_rows, head_columns), full),
            vmem((chips, proj_rows, head_columns), kind),
            vmem((chips, proj_rows, head_columns), kind),
            vmem((2, keys.shape[0], value_size), kind),
            vmem((sp_count, keys.shape[0], value_size), kind),
            vmem((all_rows, hidden_width), kind),
            vmem((all_rows, hidden_width), kind),
            vmem((all_rows, hidden_width), kind),
            vmem((tp_count - 1, sp_count, block_rows, width), kind),
            vmem((sp_count, block_rows, width), full),
            vmem((sp_count, block_rows, width), full),
            vmem((tp_count - 1, sp_count, block_rows, width), kind),
            vmem((sp_count, block_rows, width), kind),
            vmem((sp_count, block_rows, width), kind),
            dma((14,)),
            dma((12,)),
            dma((sp_count,)),
            dma((sp_count - 2, crossing)),
            dma((2, sp_count - 2)),
            dma((len(groups), crossing)),
            dma((len(groups), 2)),
            dma((tp_count - 1, 2)),
            dma((5,)),
        ],
        compiler_params=pltpu.CompilerParams(
            collective_id=0, has_side_effects=True, vmem_limit_bytes=48 * 1024 * 1024
        ),
    )(ids, group, weight, rates, queries, keys, values, mixer, cot, inp, gate, up, down, proj)


def on_device(
    cotangent,
    moe_input,
    expert_ids,
    group_weight,
    expert_weight,
    mixer_out,
    queries,
    key_vectors,
    value_vectors,
    decay_rates,
    proj_weight,
    gate_weight,
    up_weight,
    down_weight,
):
    sp_count = lax.axis_size("sp")
    tp_count = lax.axis_size("tp")
    experts_all = gate_weight.shape[0] * sp_count
    rows_here = cotangent.shape[0]
    top_count = expert_ids.shape[1]
    capacity = 3 * top_count * rows_here // (2 * experts_all)
    results = experts(
        expert_ids.T,
        group_weight[None, :],
        expert_weight.T,
        decay_rates,
        queries,
        key_vectors,
        value_vectors,
        mixer_out,
        cotangent,
        moe_input,
        gate_weight,
        up_weight,
        down_weight,
        proj_weight,
        capacity,
        sp_count,
        tp_count,
    )
    grad_gate, grad_up, grad_down, grad_proj, grad_queries, grad_keys, grad_values = store(results)
    return (
        grad_gate[None],
        grad_up[None],
        grad_down[None],
        grad_proj,
        grad_queries,
        grad_keys,
        grad_values,
    )


def solution(mesh):
    return jax.shard_map(
        on_device,
        mesh=mesh,
        in_specs=(
            P("sp", None),
            P("sp", None),
            P("sp", None),
            P("sp"),
            P("sp", None),
            P("sp", "tp"),
            P("tp", "sp"),
            P("tp", "sp"),
            P("tp", "sp"),
            P("tp", "sp"),
            P(None, "tp"),
            P("sp", None, "tp"),
            P("sp", None, "tp"),
            P("sp", "tp", None),
        ),
        out_specs=(
            P("sp", None, "tp"),
            P("sp", None, "tp"),
            P("sp", "tp", None),
            P("sp", "tp"),
            P("tp", "sp"),
            P("tp", "sp"),
            P("tp", "sp"),
        ),
        check_vma=False,
    )
```

```python
import functools

import jax
import jax.numpy as jnp
from jax import lax
from jax.experimental import pallas as pl
from jax.experimental.pallas import tpu as pltpu
from jax.sharding import PartitionSpec as P

MESH = pl.DeviceIdType.MESH
VMEM = pl.BlockSpec(memory_space=pltpu.VMEM)
ANY = pl.BlockSpec(memory_space=pl.ANY)


def partner(place, k, count):
    if k == 0:
        return place
    out = 0
    bit = 1
    while bit < count:
        b = lax.rem(place // bit, 2)
        out = out + bit * ((1 - b) if k & bit else b)
        bit *= 2
    return out


def remote(src, dst, send_sem, recv_sem, sp_place, tp_place):
    return pltpu.make_async_remote_copy(
        src_ref=src,
        dst_ref=dst,
        send_sem=send_sem,
        recv_sem=recv_sem,
        device_id={"sp": sp_place, "tp": tp_place},
        device_id_type=MESH,
    )


def state_side(here, there, count):
    return (here + count - there) // count


def dot(a, b, a_dim, b_dim):
    return lax.dot_general(
        a, b, (((a_dim,), (b_dim,)), ((), ())), preferred_element_type=jnp.float32
    )


def experts_kernel(
    sp_count, tp_count, order, groups,
    ids_hbm, group_hbm, weight_hbm, rates_hbm, queries_hbm, keys_hbm, values_hbm, mixer_hbm,
    cot_hbm, inp_hbm, gate_hbm, up_hbm, down_hbm, proj_hbm,
    grad_gate, grad_up, grad_down, grad_proj, grad_queries, grad_keys, grad_values,
    ids, group, weight, rates, queries, keys, values, mixer, cot, inp, w_gate, w_up, w_down, w_proj, picks, either, scaled, z_src, far_src, pair_src, rows, state, state_all, resid,
    scores, mixing, reaches, key_carried, proj, pair_in, proj_out, proj_in, query_out, query_all,
    hidden, gate_grad, up_grad, part, own_part, kept, summed_in, outgoing, returned,
    load_sem, send_sem, recv_z, recv_xy, recv_far, recv_rs, recv_hop, recv_ag, recv_all,
):
    me = lax.axis_index("sp")
    q = lax.axis_index("tp")
    tokens, model_width = cot.shape
    width = model_width // tp_count
    block_rows = rows.shape[2]
    hidden_width = w_gate.shape[1]
    square = tp_count == 4
    at = [partner(me, k, sp_count) for k in order]
    direct = list(range(*groups[-1])) if square else []
    peer = [partner(q, m, tp_count) for m in range(tp_count)]

    def columns(place):
        return pl.ds(pl.multiple_of(place * width, width), width)

    mine = columns(q)
    halves = 2 if width == 2 * proj.shape[2] and proj.shape[2] % 128 == 0 else 1

    def half_columns(place, j):
        size = width // halves
        return pl.ds(pl.multiple_of(place * width + j * size, size), size)

    loads = []
    for i, (src, dst) in enumerate(
        (
            (ids_hbm, ids),
            (group_hbm, group),
            (weight_hbm, weight),
            (cot_hbm, cot),
            (inp_hbm, inp),
            (rates_hbm, rates),
            (keys_hbm, keys),
            (values_hbm, values),
            (gate_hbm.at[0], w_gate),
            (up_hbm.at[0], w_up),
            (down_hbm.at[0], w_down),
            (queries_hbm, queries),
            (mixer_hbm, mixer),
            (proj_hbm, w_proj),
        )
    ):
        copy = pltpu.make_async_copy(src, dst, load_sem.at[i])
        copy.start()
        loads.append(copy)

    barrier = pltpu.get_barrier_semaphore()
    for k in range(1, sp_count):
        pl.semaphore_signal(
            barrier, inc=1, device_id={"sp": at[k], "tp": q}, device_id_type=MESH
        )
    for m in range(1, tp_count):
        pl.semaphore_signal(
            barrier, inc=1, device_id={"sp": me, "tp": peer[m]}, device_id_type=MESH
        )

    with jax.named_scope("slots"):
        for load in loads[:3]:
            load.wait()
        top_count = ids.shape[0]
        expert = lax.broadcasted_iota(jnp.int32, (sp_count, tokens), 0)
        named = [(ids[j : j + 1, :] == expert).astype(jnp.float32) for j in range(top_count)]
        earlier = lax.broadcasted_iota(jnp.int32, (tokens, tokens), 0) < lax.broadcasted_iota(
            jnp.int32, (tokens, tokens), 1
        )
        before = jnp.dot(
            sum(named).astype(jnp.bfloat16),
            earlier.astype(jnp.float32).astype(jnp.bfloat16),
            preferred_element_type=jnp.float32,
        )
        slots = []
        route = jnp.zeros((8, tokens), jnp.float32)
        lane_of = lax.broadcasted_iota(jnp.int32, (8, tokens), 0)
        for j in range(top_count):
            rank = jnp.sum(named[j] * before, axis=0, keepdims=True).astype(jnp.int32)
            before = before + named[j]
            slots.append(ids[j : j + 1, :] * block_rows + rank)
            route = jnp.where(lane_of == j, group[...] * weight[j : j + 1, :], route)
        route = jnp.transpose(route)
        row_of = lax.broadcasted_iota(jnp.int32, (block_rows, tokens), 0)
        for k in range(sp_count):
            here = pl.ds(k * block_rows, block_rows)
            pick = [(s == row_of + at[k] * block_rows).astype(jnp.float32) for s in slots]
            for j in range(top_count):
                picks[here, j * tokens : (j + 1) * tokens] = pick[j].astype(jnp.bfloat16)
            either[here, :] = sum(pick).astype(jnp.bfloat16)

    with jax.named_scope("pack"):
        loads[3].wait()
        loads[4].wait()
        cot_mine = cot[:, mine].astype(jnp.float32)
        scaled_mine = jnp.concatenate(
            [(cot_mine * route[:, j : j + 1]).astype(jnp.bfloat16) for j in range(top_count)], axis=0
        )
        first = 2 * block_rows
        cot_out = jnp.dot(picks[first:, :], scaled_mine, preferred_element_type=jnp.float32)
        inp_out = jnp.dot(either[first:, :], inp[:, mine], preferred_element_type=jnp.float32)
        for k in range(2, sp_count):
            here = slice((k - 2) * block_rows, (k - 1) * block_rows)
            z_src[k, 0] = cot_out[here].astype(z_src.dtype)
            z_src[k, 1] = inp_out[here].astype(z_src.dtype)
    with jax.named_scope("barrier"):
        pl.semaphore_wait(barrier, sp_count - 1 + tp_count - 1)

    pending = []

    def start(copy):
        copy.start()

    for k in range(2, sp_count):
        start(remote(z_src.at[k], rows.at[:, k, :, mine], send_sem.at[0], recv_z.at[k], at[k], q))
    with jax.named_scope("near"):
        cot_all = cot[...].astype(jnp.float32)
        for j in range(top_count):
            scaled[j * tokens : (j + 1) * tokens, :] = (cot_all * route[:, j : j + 1]).astype(scaled.dtype)
        cot_out = jnp.dot(picks[:first, :], scaled[...], preferred_element_type=jnp.float32)
        inp_out = jnp.dot(either[:first, :], inp[...], preferred_element_type=jnp.float32)
        pair_src[0] = cot_out[block_rows:].astype(pair_src.dtype)
        pair_src[1] = inp_out[block_rows:].astype(pair_src.dtype)
        start(remote(pair_src, rows.at[:, 1], send_sem.at[1], recv_z.at[1], at[1], q))
        if direct:
            across = columns(peer[3])
            here = slice(direct[0] * block_rows, (direct[-1] + 1) * block_rows)
            cot_far = jnp.dot(picks[here, :], scaled[:, across], preferred_element_type=jnp.float32)
            inp_far = jnp.dot(either[here, :], inp[:, across], preferred_element_type=jnp.float32)
            for i, k in enumerate(direct):
                cut = slice(i * block_rows, (i + 1) * block_rows)
                far_src[i, 0] = cot_far[cut].astype(far_src.dtype)
                far_src[i, 1] = inp_far[cut].astype(far_src.dtype)
        rows[0, 0] = cot_out[:block_rows].astype(rows.dtype)
        rows[1, 0] = inp_out[:block_rows].astype(rows.dtype)

    exact = lax.Precision.HIGHEST
    heads, length = rates.shape
    key_size = keys.shape[0] // heads
    value_size = values.shape[0] // heads
    score_scale = key_size ** (-0.5)

    def exact_dot(a, b, a_dim, b_dim):
        return lax.dot_general(
            a,
            b,
            (((a_dim,), (b_dim,)), ((), ())),
            precision=exact,
            preferred_element_type=jnp.float32,
        )

    def key_part(h):
        return slice(h * key_size, (h + 1) * key_size)

    def value_part(h):
        return slice(h * value_size, (h + 1) * value_size)

    def reach_part(h, side):
        return slice(8 * h + side, 8 * h + side + 1)

    with jax.named_scope("states"):
        for load in loads[5:8]:
            load.wait()
        upto = lax.broadcasted_iota(jnp.int32, (length, length), 0) <= lax.broadcasted_iota(
            jnp.int32, (length, length), 1
        )
        for h in range(heads):
            rate = jnp.broadcast_to(rates[h : h + 1, :], (8, length))
            prefixes = exact_dot(rate, upto.astype(jnp.float32), 1, 0)
            prefix = prefixes[0:1]
            ending = prefix[:, length - 1 : length]
            gap = jnp.transpose(prefixes)[:, 0:1] - prefix
            mixing[h] = score_scale * jnp.exp(-jnp.abs(gap))
            key = keys[key_part(h), :].astype(jnp.float32)
            value = values[value_part(h), :].astype(jnp.float32)
            top = h * (key_size + 8)
            for side, reach in enumerate((jnp.exp(prefix - ending), jnp.exp(-prefix))):
                reaches[reach_part(h, side), :] = reach
                state[side, top : top + key_size, :] = exact_dot(key * reach, value, 1, 1)
                state[side, top + key_size : top + key_size + 8, :] = jnp.broadcast_to(
                    ending, (8, value_size)
                )
        state_all[me] = state[0]
        query_all[me] = jnp.zeros(query_all.shape[1:], query_all.dtype)
        for k in range(1, sp_count):
            start(
                remote(
                    state.at[state_side(me, at[k], sp_count)],
                    state_all.at[me],
                    send_sem.at[4],
                    recv_all.at[0],
                    at[k],
                    q,
                )
            )

    def score_stage():
        loads[11].wait()
        for h in range(heads):
            query = queries[key_part(h), :].astype(jnp.float32)
            key = keys[key_part(h), :].astype(jnp.float32)
            scores[h] = mixing[h] * exact_dot(query, key, 0, 0)

    def decays(h):
        total_at = h * (key_size + 8) + key_size
        low, high = [None] * sp_count, [None] * sp_count
        totals = [state_all[b, total_at : total_at + 1, :] for b in range(sp_count)]
        run = jnp.zeros((1, value_size), jnp.float32)
        for b in reversed(range(sp_count)):
            low[b] = jnp.where(b < me, jnp.exp(-run), 0.0)
            run = run + jnp.where(b < me, totals[b], 0.0)
        run = jnp.zeros((1, value_size), jnp.float32)
        for b in range(sp_count):
            high[b] = jnp.where(b > me, jnp.exp(-run), 0.0)
            run = run + jnp.where(b > me, totals[b], 0.0)
        return low, high

    def carry_stage():
        piece = state_all.at[pl.ds(0, sp_count - 1)]
        remote(piece, piece, send_sem.at[4], recv_all.at[0], me, q).wait_recv()
        for h in range(heads):
            top = h * (key_size + 8)
            for side, decay in enumerate(decays(h)):
                total = jnp.zeros((key_size, value_size), jnp.float32)
                for b in range(sp_count):
                    total = total + decay[b] * state_all[b, top : top + key_size, :]
                key_carried[h, :, side * value_size : (side + 1) * value_size] = total

    def land(g):
        for k in range(*groups[g]):
            if k < 2:
                continue
            piece = rows.at[:, k, :, mine]
            remote(z_src.at[k], piece, send_sem.at[0], recv_z.at[k], me, q).wait_recv()
            for m in range(1, tp_count):
                if square and m == 3:
                    continue
                start(
                    remote(piece, piece, send_sem.at[2], recv_xy.at[k - 2, m - 1], me, peer[m])
                )

    def send_direct():
        for i, k in enumerate(direct):
            piece = rows.at[:, k, :, columns(peer[3])]
            start(remote(far_src.at[i], piece, send_sem.at[12], recv_far.at[0, k - 2], at[k], q))

    def relay(g):
        for k in range(*groups[g]):
            if k < 2:
                continue
            for m in range(1, tp_count):
                if square and m == 3:
                    continue
                piece = rows.at[:, k, :, columns(peer[m])]
                remote(piece, piece, send_sem.at[2], recv_xy.at[k - 2, m - 1], me, q).wait_recv()
                if square and k not in direct:
                    a = m - 1
                    half = rows.at[a, k, :, columns(peer[m])]
                    start(
                        remote(half, half, send_sem.at[3], recv_far.at[a, k - 2], me, peer[3 - m])
                    )

    def settle(g):
        for k in range(*groups[g]):
            if k == 1:
                remote(pair_src, rows.at[:, 1], send_sem.at[1], recv_z.at[1], me, q).wait_recv()
            if k in direct:
                piece = rows.at[:, k, :, columns(peer[3])]
                remote(piece, piece, send_sem.at[12], recv_far.at[0, k - 2], me, q).wait_recv()
            elif k >= 2 and square:
                for a in range(2):
                    piece = rows.at[a, k, :, columns(peer[3])]
                    remote(piece, piece, send_sem.at[3], recv_far.at[a, k - 2], me, q).wait_recv()

    def forward(g):
        low, high = groups[g]
        count = high - low
        size = count * block_rows
        here = slice(low * block_rows, high * block_rows)
        got = rows[1, low:high].reshape(size, model_width)
        gate_pre = jnp.dot(got, w_gate[...], preferred_element_type=jnp.float32)
        up_pre = jnp.dot(got, w_up[...], preferred_element_type=jnp.float32)
        sigmoid_gate = jax.nn.sigmoid(gate_pre)
        silu_gate = gate_pre * sigmoid_gate
        hidden[here, :] = (silu_gate * up_pre).astype(hidden.dtype)
        got = rows[0, low:high].reshape(size, model_width)
        hidden_grad = dot(got, w_down[...], 1, 1)
        gate_rows = (
            hidden_grad * up_pre * sigmoid_gate * (1.0 + gate_pre * (1.0 - sigmoid_gate))
        ).astype(jnp.bfloat16)
        up_rows = (hidden_grad * silu_gate).astype(jnp.bfloat16)
        gate_grad[here, :] = gate_rows
        up_grad[here, :] = up_rows

        def partial(m):
            theirs = columns(peer[m])
            total = dot(gate_rows, w_gate[theirs, :], 1, 1) + dot(up_rows, w_up[theirs, :], 1, 1)
            return total.reshape(count, block_rows, width)

        if square:
            half = count // 2
            middle = low + half
            total = partial(3).astype(part.dtype)
            part[1, low:high] = total
            total = partial(1)
            part[0, low:middle] = total[:half].astype(part.dtype)
            kept[middle:high] = total[half:]
            pending.append(first_hop(g, 0))
            total = partial(2)
            part[0, middle:high] = total[half:].astype(part.dtype)
            kept[low:middle] = total[:half]
            pending.append(first_hop(g, 1))
        else:
            for m in range(tp_count - 1, 0, -1):
                part[m - 1, low:high] = partial(m).astype(part.dtype)
                piece = pl.ds(low, count)
                start(
                    remote(
                        part.at[m - 1, piece],
                        summed_in.at[m - 1, piece],
                        send_sem.at[5],
                        recv_rs.at[g, m - 1],
                        me,
                        peer[m],
                    )
                )
        own_part[low:high] = partial(0)

    def flush():
        while pending:
            start(pending.pop(0))

    def hop_blocks(g, side):
        low, high = groups[g]
        half = (high - low) // 2
        return (low, low + half) if side == 0 else (low + half, high)

    def first_hop(g, side):
        low, high = hop_blocks(g, side)
        piece = pl.ds(low, high - low)
        return remote(
            part.at[pl.ds(0, 2), piece],
            summed_in.at[pl.ds(0, 2), piece],
            send_sem.at[5],
            recv_rs.at[g, side],
            me,
            peer[1 + side],
        )

    def second_hop(g, side):
        low, high = hop_blocks(g, side)
        piece = pl.ds(low, high - low)
        return remote(
            part.at[2, piece],
            summed_in.at[2, piece],
            send_sem.at[6],
            recv_hop.at[g, side],
            me,
            peer[2 - side],
        )

    def hop(g):
        if not square:
            return
        for side in range(2):
            low, high = hop_blocks(g, side)
            first_hop(g, side).wait_recv()
            total = kept[low:high] + summed_in[1, low:high].astype(jnp.float32)
            part[2, low:high] = total.astype(part.dtype)
            start(second_hop(g, side))

    def give_back(g):
        low, high = groups[g]
        count = high - low
        total = own_part[low:high]
        if square:
            for side in range(2):
                second_hop(g, side).wait_recv()
            total = total + summed_in[0, low:high].astype(jnp.float32)
            total = total + summed_in[2, low:high].astype(jnp.float32)
        else:
            for m in range(1, tp_count):
                piece = summed_in.at[m - 1, pl.ds(low, count)]
                remote(piece, piece, send_sem.at[5], recv_rs.at[g, m - 1], me, q).wait_recv()
                total = total + summed_in[m - 1, low:high].astype(jnp.float32)
        total = total.astype(outgoing.dtype)
        for k in range(low, high):
            if k == 0:
                returned[0] = total[0]
            else:
                outgoing[k] = total[k - low]
                start(
                    remote(
                        outgoing.at[k], returned.at[k], send_sem.at[7], recv_all.at[1], at[k], q
                    )
                )

    all_rows = sp_count * block_rows

    def down_grads():
        got = rows[0].reshape(all_rows, model_width)
        for m in range(tp_count):
            cut = slice(m * width, (m + 1) * width)
            grad_down[:, cut] = dot(hidden[...], got[:, cut], 0, 0).astype(grad_down.dtype)

    def input_grads(grads, out):
        for m in range(tp_count):
            cut = slice(m * width, (m + 1) * width)
            got = rows[1, :, :, cut].reshape(all_rows, width)
            out[cut, :] = dot(got, grads[...], 0, 0).astype(out.dtype)

    count = len(groups)
    with jax.named_scope("weights"):
        for load in loads[8:11]:
            load.wait()
    with jax.named_scope("land#g=0"):
        land(0)
        relay(0)
        settle(0)
    with jax.named_scope("forward#g=0"):
        forward(0)
    flush()
    with jax.named_scope("land#g=1"):
        land(1)
    with jax.named_scope("hop#g=0"):
        hop(0)
    send_direct()
    with jax.named_scope("relay#g=1"):
        relay(1)
    with jax.named_scope("land#g=2"):
        land(2)
    with jax.named_scope("settle#g=1"):
        settle(1)
    with jax.named_scope("forward#g=1"):
        forward(1)
    with jax.named_scope("relay#g=2"):
        relay(2)
    flush()
    with jax.named_scope("settle#g=2"):
        settle(2)
    with jax.named_scope("land#g=3"):
        land(3)
    with jax.named_scope("hop#g=1"):
        hop(1)
    with jax.named_scope("forward#g=2"):
        forward(2)
    flush()
    with jax.named_scope("give#g=0"):
        give_back(0)
    with jax.named_scope("relay#g=3"):
        relay(3)
    with jax.named_scope("settle#g=3"):
        settle(3)
    with jax.named_scope("forward#g=3"):
        forward(3)
    with jax.named_scope("hop#g=2"):
        hop(2)
    flush()
    with jax.named_scope("give#g=1"):
        give_back(1)
    with jax.named_scope("grad_down"):
        down_grads()
    with jax.named_scope("give#g=2"):
        give_back(2)
    with jax.named_scope("hop#g=3"):
        hop(3)
    with jax.named_scope("grad_gate"):
        input_grads(gate_grad, grad_gate)
    with jax.named_scope("give#g=3"):
        give_back(3)
    with jax.named_scope("carry"):
        score_stage()
        carry_stage()
    with jax.named_scope("back"):
        piece = returned.at[pl.ds(0, sp_count - 1)]
        remote(piece, piece, send_sem.at[7], recv_all.at[1], me, q).wait_recv()
    with jax.named_scope("combine"):
        total = dot(either[...], returned[...].reshape(all_rows, width), 0, 0)
        resid[:, mine] = (cot[:, mine].astype(jnp.float32) + total).astype(resid.dtype)
        for j in range(halves):
            piece = resid.at[:, half_columns(q, j)]
            for m in range(tp_count - 1, 0, -1):
                start(remote(piece, piece, send_sem.at[8], recv_ag.at[m - 1, j], me, peer[m]))

    core = lax.rem(me, 2)
    chips_here = width // (2 * proj.shape[2])

    def project(m, j):
        piece = resid[:, half_columns(peer[m], j)]
        part_here = dot(piece, mixer[...], 0, 0)
        chips = pl.ds(peer[m] * chips_here, chips_here)
        if halves == 2:
            proj[chips, j] = part_here.reshape((chips_here,) + proj.shape[2:])
        else:
            proj[chips] = part_here.reshape((chips_here,) + proj.shape[1:])
        return dot(w_proj[half_columns(peer[m], j), :], piece, 0, 1)

    def pair_copy():
        return remote(
            proj.at[:, 1 - core], pair_in, send_sem.at[9], recv_all.at[2], at[1], q
        )

    def pair_total(chip):
        return proj[chip, core] + pair_in[chip]

    def across_chips():
        pair_copy().wait_recv()
        for k in reversed(range(2, sp_count, 2)):
            proj_out[k // 2] = pair_total(at[k] // 2).astype(proj_out.dtype)
            start(
                remote(
                    proj_out.at[k // 2],
                    proj_in.at[k // 2],
                    send_sem.at[10],
                    recv_all.at[3],
                    at[k],
                    q,
                )
            )
        grad_proj[...] = pair_total(me // 2)

    with jax.named_scope("project#m=0"):
        loads[12].wait()
        loads[13].wait()
        out_grad = project(0, 0)
        for j in range(1, halves):
            out_grad = out_grad + project(0, j)
    with jax.named_scope("grad_up"):
        input_grads(up_grad, grad_up)
    for j in range(halves):
        for m in range(1, tp_count):
            with jax.named_scope(f"gather#m={m}#j={j}"):
                piece = resid.at[:, half_columns(peer[m], j)]
                remote(piece, piece, send_sem.at[8], recv_ag.at[m - 1, j], me, q).wait_recv()
            with jax.named_scope(f"project#m={m}#j={j}"):
                out_grad = out_grad + project(m, j)
        if halves == 2:
            with jax.named_scope(f"pair#j={j}"):

                @pl.when(core != j)
                def _():
                    pair_copy().start()

                if j == 0:

                    @pl.when(core == j)
                    def _():
                        across_chips()

    if halves == 1:
        pair_copy().start()
    with jax.named_scope("query_states"):
        for h in range(heads):
            query = queries[key_part(h), :].astype(jnp.float32)
            for side in range(2):
                seen = exact_dot(query * reaches[reach_part(h, side), :], out_grad[value_part(h)], 1, 1)
                query_out[side, key_part(h), :] = seen.astype(query_out.dtype)
        for k in reversed(range(1, sp_count)):
            start(
                remote(
                    query_out.at[state_side(me, at[k], sp_count)],
                    query_all.at[me],
                    send_sem.at[11],
                    recv_all.at[4],
                    at[k],
                    q,
                )
            )
    with jax.named_scope("pair"):
        if halves == 1:
            across_chips()
        else:

            @pl.when(core == 1)
            def _():
                across_chips()

    with jax.named_scope("retention"):
        for h in range(heads):
            query = queries[key_part(h), :].astype(jnp.float32)
            key = keys[key_part(h), :].astype(jnp.float32)
            value = values[value_part(h), :].astype(jnp.float32)
            grad = out_grad[value_part(h)]
            score_grad = mixing[h] * exact_dot(grad, value, 0, 0)
            to_end = score_scale * reaches[reach_part(h, 0), :]
            from_start = score_scale * reaches[reach_part(h, 1), :]
            out_reach = jnp.concatenate([grad * from_start, grad * to_end], axis=0)
            grad_queries[key_part(h), :] = exact_dot(key, score_grad, 1, 1) + exact_dot(
                key_carried[h], out_reach, 1, 0
            )
            grad_keys[key_part(h), :] = exact_dot(query, score_grad, 1, 0)
            grad_values[value_part(h), :] = exact_dot(grad, scores[h], 1, 0)
    with jax.named_scope("query_wait"):
        piece = query_all.at[pl.ds(0, sp_count - 1)]
        remote(piece, piece, send_sem.at[11], recv_all.at[4], me, q).wait_recv()
    with jax.named_scope("finish"):
        for h in range(heads):
            key = keys[key_part(h), :].astype(jnp.float32)
            value = values[value_part(h), :].astype(jnp.float32)
            to_end = score_scale * reaches[reach_part(h, 0), :]
            from_start = score_scale * reaches[reach_part(h, 1), :]
            carried = []
            for decay in decays(h):
                total = jnp.zeros((key_size, value_size), jnp.float32)
                for b in range(sp_count):
                    total = total + decay[b] * query_all[b, key_part(h), :].astype(jnp.float32)
                carried.append(total)
            value_reach = jnp.concatenate([value * from_start, value * to_end], axis=0)
            key_reach = jnp.concatenate([key * from_start, key * to_end], axis=0)
            grad_keys[key_part(h), :] = grad_keys[key_part(h), :] + exact_dot(
                jnp.concatenate(carried, axis=1), value_reach, 1, 0
            )
            grad_values[value_part(h), :] = grad_values[value_part(h), :] + exact_dot(
                jnp.concatenate(carried, axis=0), key_reach, 0, 0
            )
    with jax.named_scope("proj_wait"):
        piece = proj_in.at[pl.ds(1, sp_count // 2 - 1)]
        remote(piece, piece, send_sem.at[10], recv_all.at[3], me, q).wait_recv()
        proj_total = grad_proj[...]
        for i in range(1, sp_count // 2):
            proj_total = proj_total + proj_in[i].astype(jnp.float32)
        grad_proj[...] = proj_total
    with jax.named_scope("sent"):
        others = pl.ds(0, sp_count - 2)
        crossing = 2 if square else tp_count - 1
        sent = [
            rows.at[:, others, :, pl.ds(0, width)],
            pair_src,
            rows.at[:, others, :, pl.ds(0, crossing * width)],
            rows.at[:, pl.ds(0, sp_count - 2 - len(direct)), :, pl.ds(0, width)] if square else None,
            state_all.at[pl.ds(0, sp_count - 1)],
            part.at[pl.ds(0, 2)] if square else part,
            part.at[2] if square else None,
            outgoing.at[pl.ds(0, sp_count - 1)],
            resid.at[:, pl.ds(0, (tp_count - 1) * width)],
            pair_in,
            proj_out.at[pl.ds(0, sp_count // 2 - 1)],
            query_all.at[pl.ds(0, sp_count - 1)],
            rows.at[:, pl.ds(0, len(direct)), :, pl.ds(0, width)] if square else None,
        ]
        for i, piece in enumerate(sent):
            if piece is not None:
                remote(piece, piece, send_sem.at[i], recv_all.at[0], me, q).wait_send()


def store_kernel(*refs):
    count = (len(refs) - 1) // 2
    copies = [
        pltpu.make_async_copy(refs[i], refs[count + i], refs[-1].at[i]) for i in range(count)
    ]
    for copy in copies:
        copy.start()
    for copy in copies:
        copy.wait()


def store(arrays):
    return pl.pallas_call(
        store_kernel,
        out_shape=tuple(jax.ShapeDtypeStruct(a.shape, a.dtype) for a in arrays),
        in_specs=[VMEM] * len(arrays),
        out_specs=(ANY,) * len(arrays),
        scratch_shapes=[pltpu.SemaphoreType.DMA((len(arrays),))],
        compiler_params=pltpu.CompilerParams(vmem_limit_bytes=16 * 1024 * 1024),
    )(*arrays)


def experts(
    ids, group, weight, rates, queries, keys, values, mixer, cot, inp, gate, up, down, proj, capacity, sp_count, tp_count
):
    tokens, model_width = cot.shape
    width = model_width // tp_count
    hidden_width = gate.shape[2]
    heads, length = rates.shape
    state_rows = keys.shape[0] + 8 * heads
    key_size = keys.shape[0] // heads
    value_size = values.shape[0] // heads
    head_columns = mixer.shape[1]
    proj_rows = model_width // sp_count
    block_rows = -(-capacity // 16) * 16
    all_rows = sp_count * block_rows
    chips = sp_count // 2
    quarter = sp_count // 4
    pairs = [0, 1] + list(range(sp_count // 2 - 1, 1, -1))
    order = [k for pair in pairs for k in (2 * pair, 2 * pair + 1)]
    groups = [(i * quarter, (i + 1) * quarter) for i in range(4)]
    crossing = 2 if tp_count == 4 else tp_count - 1
    kind = cot.dtype
    full = jnp.float32
    dma = pltpu.SemaphoreType.DMA
    vmem = pltpu.VMEM
    return pl.pallas_call(
        functools.partial(experts_kernel, sp_count, tp_count, order, groups),
        out_shape=(
            vmem((model_width, hidden_width), kind),
            vmem((model_width, hidden_width), kind),
            vmem((hidden_width, model_width), kind),
            vmem((proj_rows, head_columns), full),
            vmem(queries.shape, full),
            vmem(keys.shape, full),
            vmem(values.shape, full),
        ),
        in_specs=[ANY] * 14,
        out_specs=(VMEM,) * 7,
        scratch_shapes=[
            vmem(ids.shape, ids.dtype),
            vmem(group.shape, group.dtype),
            vmem(weight.shape, weight.dtype),
            vmem(rates.shape, rates.dtype),
            vmem(queries.shape, queries.dtype),
            vmem(keys.shape, keys.dtype),
            vmem(values.shape, values.dtype),
            vmem(mixer.shape, mixer.dtype),
            vmem((tokens, model_width), kind),
            vmem((tokens, model_width), kind),
            vmem((model_width, hidden_width), kind),
            vmem((model_width, hidden_width), kind),
            vmem((hidden_width, model_width), kind),
            vmem(proj.shape, kind),
            vmem((all_rows, ids.shape[0] * tokens), jnp.bfloat16),
            vmem((all_rows, tokens), jnp.bfloat16),
            vmem((ids.shape[0] * tokens, model_width), kind),
            vmem((sp_count, 2, block_rows, width), kind),
            vmem((quarter, 2, block_rows, width), kind),
            vmem((2, block_rows, model_width), kind),
            vmem((2, sp_count, block_rows, model_width), kind),
            vmem((2, state_rows, value_size), full),
            vmem((sp_count, state_rows, value_size), full),
            vmem((tokens, model_width), kind),
            vmem((heads, length, length), full),
            vmem((heads, length, length), full),
            vmem((8 * heads, length), full),
            vmem((heads, key_size, 2 * value_size), full),
            vmem((chips, 2, proj_rows, head_columns), full),
            vmem((chips, proj_rows, head_columns), full),
            vmem((chips, proj_rows, head_columns), kind),
            vmem((chips, proj_rows, head_columns), kind),
            vmem((2, keys.shape[0], value_size), kind),
            vmem((sp_count, keys.shape[0], value_size), kind),
            vmem((all_rows, hidden_width), kind),
            vmem((all_rows, hidden_width), kind),
            vmem((all_rows, hidden_width), kind),
            vmem((tp_count - 1, sp_count, block_rows, width), kind),
            vmem((sp_count, block_rows, width), full),
            vmem((sp_count, block_rows, width), full),
            vmem((tp_count - 1, sp_count, block_rows, width), kind),
            vmem((sp_count, block_rows, width), kind),
            vmem((sp_count, block_rows, width), kind),
            dma((14,)),
            dma((13,)),
            dma((sp_count,)),
            dma((sp_count - 2, crossing)),
            dma((2, sp_count - 2)),
            dma((len(groups), crossing)),
            dma((len(groups), 2)),
            dma((tp_count - 1, 2)),
            dma((5,)),
        ],
        compiler_params=pltpu.CompilerParams(
            collective_id=0, has_side_effects=True, vmem_limit_bytes=48 * 1024 * 1024
        ),
    )(ids, group, weight, rates, queries, keys, values, mixer, cot, inp, gate, up, down, proj)


def on_device(
    cotangent,
    moe_input,
    expert_ids,
    group_weight,
    expert_weight,
    mixer_out,
    queries,
    key_vectors,
    value_vectors,
    decay_rates,
    proj_weight,
    gate_weight,
    up_weight,
    down_weight,
):
    sp_count = lax.axis_size("sp")
    tp_count = lax.axis_size("tp")
    experts_all = gate_weight.shape[0] * sp_count
    rows_here = cotangent.shape[0]
    top_count = expert_ids.shape[1]
    capacity = 3 * top_count * rows_here // (2 * experts_all)
    results = experts(
        expert_ids.T,
        group_weight[None, :],
        expert_weight.T,
        decay_rates,
        queries,
        key_vectors,
        value_vectors,
        mixer_out,
        cotangent,
        moe_input,
        gate_weight,
        up_weight,
        down_weight,
        proj_weight,
        capacity,
        sp_count,
        tp_count,
    )
    grad_gate, grad_up, grad_down, grad_proj, grad_queries, grad_keys, grad_values = store(results)
    return (
        grad_gate[None],
        grad_up[None],
        grad_down[None],
        grad_proj,
        grad_queries,
        grad_keys,
        grad_values,
    )


def solution(mesh):
    return jax.shard_map(
        on_device,
        mesh=mesh,
        in_specs=(
            P("sp", None),
            P("sp", None),
            P("sp", None),
            P("sp"),
            P("sp", None),
            P("sp", "tp"),
            P("tp", "sp"),
            P("tp", "sp"),
            P("tp", "sp"),
            P("tp", "sp"),
            P(None, "tp"),
            P("sp", None, "tp"),
            P("sp", None, "tp"),
            P("sp", "tp", None),
        ),
        out_specs=(
            P("sp", None, "tp"),
            P("sp", None, "tp"),
            P("sp", "tp", None),
            P("sp", "tp"),
            P("tp", "sp"),
            P("tp", "sp"),
            P("tp", "sp"),
        ),
        check_vma=False,
    )
```

```python
import functools

import jax
import jax.numpy as jnp
from jax import lax
from jax.experimental import pallas as pl
from jax.experimental.pallas import tpu as pltpu
from jax.sharding import PartitionSpec as P

MESH = pl.DeviceIdType.MESH
VMEM = pl.BlockSpec(memory_space=pltpu.VMEM)
ANY = pl.BlockSpec(memory_space=pl.ANY)


def partner(place, k, count):
    if k == 0:
        return place
    out = 0
    bit = 1
    while bit < count:
        b = lax.rem(place // bit, 2)
        out = out + bit * ((1 - b) if k & bit else b)
        bit *= 2
    return out


def remote(src, dst, send_sem, recv_sem, sp_place, tp_place):
    return pltpu.make_async_remote_copy(
        src_ref=src,
        dst_ref=dst,
        send_sem=send_sem,
        recv_sem=recv_sem,
        device_id={"sp": sp_place, "tp": tp_place},
        device_id_type=MESH,
    )


def state_side(here, there, count):
    return (here + count - there) // count


def dot(a, b, a_dim, b_dim):
    return lax.dot_general(
        a, b, (((a_dim,), (b_dim,)), ((), ())), preferred_element_type=jnp.float32
    )


def experts_kernel(
    sp_count, tp_count, order, groups,
    ids_hbm, group_hbm, weight_hbm, rates_hbm, queries_hbm, keys_hbm, values_hbm, mixer_hbm,
    cot_hbm, inp_hbm, gate_hbm, up_hbm, down_hbm, proj_hbm,
    grad_gate, grad_up, grad_down, grad_proj, grad_queries, grad_keys, grad_values,
    ids, group, weight, rates, queries, keys, values, mixer, cot, inp, w_gate, w_up, w_down, w_proj, picks, either, scaled, z_src, far_src, pair_src, rows, state, state_all, resid,
    scores, mixing, reaches, key_carried, proj, pair_in, proj_out, proj_in, query_out, query_all,
    hidden, gate_grad, up_grad, part, own_part, kept, summed_in, outgoing, returned,
    load_sem, send_sem, recv_z, recv_xy, recv_far, recv_rs, recv_hop, recv_ag, recv_all,
):
    me = lax.axis_index("sp")
    q = lax.axis_index("tp")
    tokens, model_width = cot.shape
    width = model_width // tp_count
    block_rows = rows.shape[2]
    hidden_width = w_gate.shape[1]
    square = tp_count == 4
    at = [partner(me, k, sp_count) for k in order]
    direct = list(range(*groups[-1])) if square else []
    peer = [partner(q, m, tp_count) for m in range(tp_count)]

    def columns(place):
        return pl.ds(pl.multiple_of(place * width, width), width)

    mine = columns(q)
    halves = 2 if width == 2 * proj.shape[2] and proj.shape[2] % 128 == 0 else 1

    def half_columns(place, j):
        size = width // halves
        return pl.ds(pl.multiple_of(place * width + j * size, size), size)

    loads = []
    for i, (src, dst) in enumerate(
        (
            (ids_hbm, ids),
            (group_hbm, group),
            (weight_hbm, weight),
            (cot_hbm, cot),
            (inp_hbm, inp),
            (rates_hbm, rates),
            (keys_hbm, keys),
            (values_hbm, values),
            (gate_hbm.at[0], w_gate),
            (up_hbm.at[0], w_up),
            (down_hbm.at[0], w_down),
            (queries_hbm, queries),
            (mixer_hbm, mixer),
            (proj_hbm, w_proj),
        )
    ):
        copy = pltpu.make_async_copy(src, dst, load_sem.at[i])
        copy.start()
        loads.append(copy)

    barrier = pltpu.get_barrier_semaphore()
    for k in range(1, sp_count):
        pl.semaphore_signal(
            barrier, inc=1, device_id={"sp": at[k], "tp": q}, device_id_type=MESH
        )
    for m in range(1, tp_count):
        pl.semaphore_signal(
            barrier, inc=1, device_id={"sp": me, "tp": peer[m]}, device_id_type=MESH
        )

    with jax.named_scope("slots"):
        for load in loads[:3]:
            load.wait()
        top_count = ids.shape[0]
        expert = lax.broadcasted_iota(jnp.int32, (sp_count, tokens), 0)
        named = [(ids[j : j + 1, :] == expert).astype(jnp.float32) for j in range(top_count)]
        earlier = lax.broadcasted_iota(jnp.int32, (tokens, tokens), 0) < lax.broadcasted_iota(
            jnp.int32, (tokens, tokens), 1
        )
        before = jnp.dot(
            sum(named).astype(jnp.bfloat16),
            earlier.astype(jnp.float32).astype(jnp.bfloat16),
            preferred_element_type=jnp.float32,
        )
        slots = []
        route = jnp.zeros((8, tokens), jnp.float32)
        lane_of = lax.broadcasted_iota(jnp.int32, (8, tokens), 0)
        for j in range(top_count):
            rank = jnp.sum(named[j] * before, axis=0, keepdims=True).astype(jnp.int32)
            before = before + named[j]
            slots.append(ids[j : j + 1, :] * block_rows + rank)
            route = jnp.where(lane_of == j, group[...] * weight[j : j + 1, :], route)
        route = jnp.transpose(route)
        row_of = lax.broadcasted_iota(jnp.int32, (block_rows, tokens), 0)
        for k in range(sp_count):
            here = pl.ds(k * block_rows, block_rows)
            pick = [(s == row_of + at[k] * block_rows).astype(jnp.float32) for s in slots]
            for j in range(top_count):
                picks[here, j * tokens : (j + 1) * tokens] = pick[j].astype(jnp.bfloat16)
            either[here, :] = sum(pick).astype(jnp.bfloat16)

    with jax.named_scope("pack"):
        loads[3].wait()
        loads[4].wait()
        cot_mine = cot[:, mine].astype(jnp.float32)
        scaled_mine = jnp.concatenate(
            [(cot_mine * route[:, j : j + 1]).astype(jnp.bfloat16) for j in range(top_count)], axis=0
        )
        first = 2 * block_rows
        cot_out = jnp.dot(picks[first:, :], scaled_mine, preferred_element_type=jnp.float32)
        inp_out = jnp.dot(either[first:, :], inp[:, mine], preferred_element_type=jnp.float32)
        for k in range(2, sp_count):
            here = slice((k - 2) * block_rows, (k - 1) * block_rows)
            z_src[k, 0] = cot_out[here].astype(z_src.dtype)
            z_src[k, 1] = inp_out[here].astype(z_src.dtype)
    with jax.named_scope("barrier"):
        pl.semaphore_wait(barrier, sp_count - 1 + tp_count - 1)

    pending = []

    def start(copy):
        copy.start()

    for k in range(2, sp_count):
        start(remote(z_src.at[k], rows.at[:, k, :, mine], send_sem.at[0], recv_z.at[k], at[k], q))
    with jax.named_scope("near"):
        cot_all = cot[...].astype(jnp.float32)
        for j in range(top_count):
            scaled[j * tokens : (j + 1) * tokens, :] = (cot_all * route[:, j : j + 1]).astype(scaled.dtype)
        cot_out = jnp.dot(picks[:first, :], scaled[...], preferred_element_type=jnp.float32)
        inp_out = jnp.dot(either[:first, :], inp[...], preferred_element_type=jnp.float32)
        pair_src[0] = cot_out[block_rows:].astype(pair_src.dtype)
        pair_src[1] = inp_out[block_rows:].astype(pair_src.dtype)
        start(remote(pair_src, rows.at[:, 1], send_sem.at[1], recv_z.at[1], at[1], q))
        if direct:
            across = columns(peer[3])
            here = slice(direct[0] * block_rows, (direct[-1] + 1) * block_rows)
            cot_far = jnp.dot(picks[here, :], scaled[:, across], preferred_element_type=jnp.float32)
            inp_far = jnp.dot(either[here, :], inp[:, across], preferred_element_type=jnp.float32)
            for i, k in enumerate(direct):
                cut = slice(i * block_rows, (i + 1) * block_rows)
                far_src[i, 0] = cot_far[cut].astype(far_src.dtype)
                far_src[i, 1] = inp_far[cut].astype(far_src.dtype)
        rows[0, 0] = cot_out[:block_rows].astype(rows.dtype)
        rows[1, 0] = inp_out[:block_rows].astype(rows.dtype)

    exact = lax.Precision.HIGHEST
    heads, length = rates.shape
    key_size = keys.shape[0] // heads
    value_size = values.shape[0] // heads
    score_scale = key_size ** (-0.5)

    def exact_dot(a, b, a_dim, b_dim):
        return lax.dot_general(
            a,
            b,
            (((a_dim,), (b_dim,)), ((), ())),
            precision=exact,
            preferred_element_type=jnp.float32,
        )

    def key_part(h):
        return slice(h * key_size, (h + 1) * key_size)

    def value_part(h):
        return slice(h * value_size, (h + 1) * value_size)

    def reach_part(h, side):
        return slice(8 * h + side, 8 * h + side + 1)

    with jax.named_scope("states"):
        for load in loads[5:8]:
            load.wait()
        upto = lax.broadcasted_iota(jnp.int32, (length, length), 0) <= lax.broadcasted_iota(
            jnp.int32, (length, length), 1
        )
        for h in range(heads):
            rate = jnp.broadcast_to(rates[h : h + 1, :], (8, length))
            prefixes = exact_dot(rate, upto.astype(jnp.float32), 1, 0)
            prefix = prefixes[0:1]
            ending = prefix[:, length - 1 : length]
            gap = jnp.transpose(prefixes)[:, 0:1] - prefix
            mixing[h] = score_scale * jnp.exp(-jnp.abs(gap))
            key = keys[key_part(h), :].astype(jnp.float32)
            value = values[value_part(h), :].astype(jnp.float32)
            top = h * (key_size + 8)
            for side, reach in enumerate((jnp.exp(prefix - ending), jnp.exp(-prefix))):
                reaches[reach_part(h, side), :] = reach
                state[side, top : top + key_size, :] = exact_dot(key * reach, value, 1, 1)
                state[side, top + key_size : top + key_size + 8, :] = jnp.broadcast_to(
                    ending, (8, value_size)
                )
        state_all[me] = state[0]
        query_all[me] = jnp.zeros(query_all.shape[1:], query_all.dtype)
        for k in range(1, sp_count):
            start(
                remote(
                    state.at[state_side(me, at[k], sp_count)],
                    state_all.at[me],
                    send_sem.at[4],
                    recv_all.at[0],
                    at[k],
                    q,
                )
            )

    def score_stage():
        loads[11].wait()
        for h in range(heads):
            query = queries[key_part(h), :].astype(jnp.float32)
            key = keys[key_part(h), :].astype(jnp.float32)
            scores[h] = mixing[h] * exact_dot(query, key, 0, 0)

    def decays(h):
        total_at = h * (key_size + 8) + key_size
        low, high = [None] * sp_count, [None] * sp_count
        totals = [state_all[b, total_at : total_at + 1, :] for b in range(sp_count)]
        run = jnp.zeros((1, value_size), jnp.float32)
        for b in reversed(range(sp_count)):
            low[b] = jnp.where(b < me, jnp.exp(-run), 0.0)
            run = run + jnp.where(b < me, totals[b], 0.0)
        run = jnp.zeros((1, value_size), jnp.float32)
        for b in range(sp_count):
            high[b] = jnp.where(b > me, jnp.exp(-run), 0.0)
            run = run + jnp.where(b > me, totals[b], 0.0)
        return low, high

    def carry_stage():
        piece = state_all.at[pl.ds(0, sp_count - 1)]
        remote(piece, piece, send_sem.at[4], recv_all.at[0], me, q).wait_recv()
        for h in range(heads):
            top = h * (key_size + 8)
            for side, decay in enumerate(decays(h)):
                total = jnp.zeros((key_size, value_size), jnp.float32)
                for b in range(sp_count):
                    total = total + decay[b] * state_all[b, top : top + key_size, :]
                key_carried[h, :, side * value_size : (side + 1) * value_size] = total

    def land(g):
        for k in range(*groups[g]):
            if k < 2:
                continue
            piece = rows.at[:, k, :, mine]
            remote(z_src.at[k], piece, send_sem.at[0], recv_z.at[k], me, q).wait_recv()
            for m in range(1, tp_count):
                if square and m == 3:
                    continue
                start(
                    remote(piece, piece, send_sem.at[2], recv_xy.at[k - 2, m - 1], me, peer[m])
                )

    def send_direct():
        for i, k in enumerate(direct):
            piece = rows.at[:, k, :, columns(peer[3])]
            start(remote(far_src.at[i], piece, send_sem.at[12], recv_far.at[0, k - 2], at[k], q))

    def relay(g):
        for k in range(*groups[g]):
            if k < 2:
                continue
            for m in range(1, tp_count):
                if square and m == 3:
                    continue
                piece = rows.at[:, k, :, columns(peer[m])]
                remote(piece, piece, send_sem.at[2], recv_xy.at[k - 2, m - 1], me, q).wait_recv()
                if square and k not in direct:
                    a = m - 1
                    half = rows.at[a, k, :, columns(peer[m])]
                    start(
                        remote(half, half, send_sem.at[3], recv_far.at[a, k - 2], me, peer[3 - m])
                    )

    def settle(g):
        for k in range(*groups[g]):
            if k == 1:
                remote(pair_src, rows.at[:, 1], send_sem.at[1], recv_z.at[1], me, q).wait_recv()
            if k in direct:
                piece = rows.at[:, k, :, columns(peer[3])]
                remote(piece, piece, send_sem.at[12], recv_far.at[0, k - 2], me, q).wait_recv()
            elif k >= 2 and square:
                for a in range(2):
                    piece = rows.at[a, k, :, columns(peer[3])]
                    remote(piece, piece, send_sem.at[3], recv_far.at[a, k - 2], me, q).wait_recv()

    def forward(g):
        low, high = groups[g]
        count = high - low
        size = count * block_rows
        here = slice(low * block_rows, high * block_rows)
        got = rows[1, low:high].reshape(size, model_width)
        gate_pre = jnp.dot(got, w_gate[...], preferred_element_type=jnp.float32)
        up_pre = jnp.dot(got, w_up[...], preferred_element_type=jnp.float32)
        sigmoid_gate = jax.nn.sigmoid(gate_pre)
        silu_gate = gate_pre * sigmoid_gate
        hidden[here, :] = (silu_gate * up_pre).astype(hidden.dtype)
        got = rows[0, low:high].reshape(size, model_width)
        hidden_grad = dot(got, w_down[...], 1, 1)
        gate_rows = (
            hidden_grad * up_pre * sigmoid_gate * (1.0 + gate_pre * (1.0 - sigmoid_gate))
        ).astype(jnp.bfloat16)
        up_rows = (hidden_grad * silu_gate).astype(jnp.bfloat16)
        gate_grad[here, :] = gate_rows
        up_grad[here, :] = up_rows

        def partial(m):
            theirs = columns(peer[m])
            total = dot(gate_rows, w_gate[theirs, :], 1, 1) + dot(up_rows, w_up[theirs, :], 1, 1)
            return total.reshape(count, block_rows, width)

        if square:
            half = count // 2
            middle = low + half
            total = partial(3).astype(part.dtype)
            part[1, low:high] = total
            total = partial(1)
            part[0, low:middle] = total[:half].astype(part.dtype)
            kept[middle:high] = total[half:]
            pending.append(first_hop(g, 0))
            total = partial(2)
            part[0, middle:high] = total[half:].astype(part.dtype)
            kept[low:middle] = total[:half]
            pending.append(first_hop(g, 1))
        else:
            for m in range(tp_count - 1, 0, -1):
                part[m - 1, low:high] = partial(m).astype(part.dtype)
                piece = pl.ds(low, count)
                start(
                    remote(
                        part.at[m - 1, piece],
                        summed_in.at[m - 1, piece],
                        send_sem.at[5],
                        recv_rs.at[g, m - 1],
                        me,
                        peer[m],
                    )
                )
        own_part[low:high] = partial(0)

    def flush():
        while pending:
            start(pending.pop(0))

    def hop_blocks(g, side):
        low, high = groups[g]
        half = (high - low) // 2
        return (low, low + half) if side == 0 else (low + half, high)

    def first_hop(g, side):
        low, high = hop_blocks(g, side)
        piece = pl.ds(low, high - low)
        return remote(
            part.at[pl.ds(0, 2), piece],
            summed_in.at[pl.ds(0, 2), piece],
            send_sem.at[5],
            recv_rs.at[g, side],
            me,
            peer[1 + side],
        )

    def second_hop(g, side):
        low, high = hop_blocks(g, side)
        piece = pl.ds(low, high - low)
        return remote(
            part.at[2, piece],
            summed_in.at[2, piece],
            send_sem.at[6],
            recv_hop.at[g, side],
            me,
            peer[2 - side],
        )

    def hop(g):
        if not square:
            return
        for side in range(2):
            low, high = hop_blocks(g, side)
            first_hop(g, side).wait_recv()
            total = kept[low:high] + summed_in[1, low:high].astype(jnp.float32)
            part[2, low:high] = total.astype(part.dtype)
            start(second_hop(g, side))

    def give_back(g):
        low, high = groups[g]
        count = high - low
        total = own_part[low:high]
        if square:
            for side in range(2):
                second_hop(g, side).wait_recv()
            total = total + summed_in[0, low:high].astype(jnp.float32)
            total = total + summed_in[2, low:high].astype(jnp.float32)
        else:
            for m in range(1, tp_count):
                piece = summed_in.at[m - 1, pl.ds(low, count)]
                remote(piece, piece, send_sem.at[5], recv_rs.at[g, m - 1], me, q).wait_recv()
                total = total + summed_in[m - 1, low:high].astype(jnp.float32)
        total = total.astype(outgoing.dtype)
        for k in range(low, high):
            if k == 0:
                returned[0] = total[0]
            else:
                outgoing[k] = total[k - low]
                start(
                    remote(
                        outgoing.at[k], returned.at[k], send_sem.at[7], recv_all.at[1], at[k], q
                    )
                )

    all_rows = sp_count * block_rows

    def down_grads():
        got = rows[0].reshape(all_rows, model_width)
        for m in range(tp_count):
            cut = slice(m * width, (m + 1) * width)
            grad_down[:, cut] = dot(hidden[...], got[:, cut], 0, 0).astype(grad_down.dtype)

    def input_grads(grads, out):
        for m in range(tp_count):
            cut = slice(m * width, (m + 1) * width)
            got = rows[1, :, :, cut].reshape(all_rows, width)
            out[cut, :] = dot(got, grads[...], 0, 0).astype(out.dtype)

    count = len(groups)
    with jax.named_scope("weights"):
        for load in loads[8:11]:
            load.wait()
    with jax.named_scope("land#g=0"):
        land(0)
        relay(0)
        settle(0)
    with jax.named_scope("forward#g=0"):
        forward(0)
    flush()
    with jax.named_scope("land#g=1"):
        land(1)
    with jax.named_scope("hop#g=0"):
        hop(0)
    send_direct()
    with jax.named_scope("relay#g=1"):
        relay(1)
    with jax.named_scope("land#g=2"):
        land(2)
    with jax.named_scope("settle#g=1"):
        settle(1)
    with jax.named_scope("forward#g=1"):
        forward(1)
    with jax.named_scope("relay#g=2"):
        relay(2)
    flush()
    with jax.named_scope("settle#g=2"):
        settle(2)
    with jax.named_scope("land#g=3"):
        land(3)
    with jax.named_scope("hop#g=1"):
        hop(1)
    with jax.named_scope("forward#g=2"):
        forward(2)
    flush()
    with jax.named_scope("give#g=0"):
        give_back(0)
    with jax.named_scope("relay#g=3"):
        relay(3)
    with jax.named_scope("settle#g=3"):
        settle(3)
    with jax.named_scope("forward#g=3"):
        forward(3)
    with jax.named_scope("hop#g=2"):
        hop(2)
    flush()
    with jax.named_scope("give#g=1"):
        give_back(1)
    with jax.named_scope("grad_down"):
        down_grads()
    with jax.named_scope("give#g=2"):
        give_back(2)
    with jax.named_scope("hop#g=3"):
        hop(3)
    with jax.named_scope("grad_gate"):
        input_grads(gate_grad, grad_gate)
    with jax.named_scope("carry"):
        score_stage()
        carry_stage()
    with jax.named_scope("give#g=3"):
        give_back(3)
    with jax.named_scope("back"):
        piece = returned.at[pl.ds(0, sp_count - 1)]
        remote(piece, piece, send_sem.at[7], recv_all.at[1], me, q).wait_recv()
    with jax.named_scope("combine"):
        total = dot(either[...], returned[...].reshape(all_rows, width), 0, 0)
        resid[:, mine] = (cot[:, mine].astype(jnp.float32) + total).astype(resid.dtype)
        for j in range(halves):
            piece = resid.at[:, half_columns(q, j)]
            for m in range(tp_count - 1, 0, -1):
                start(remote(piece, piece, send_sem.at[8], recv_ag.at[m - 1, j], me, peer[m]))

    core = lax.rem(me, 2)
    chips_here = width // (2 * proj.shape[2])

    def project(m, j):
        piece = resid[:, half_columns(peer[m], j)]
        part_here = dot(piece, mixer[...], 0, 0)
        chips = pl.ds(peer[m] * chips_here, chips_here)
        if halves == 2:
            proj[chips, j] = part_here.reshape((chips_here,) + proj.shape[2:])
        else:
            proj[chips] = part_here.reshape((chips_here,) + proj.shape[1:])
        return dot(w_proj[half_columns(peer[m], j), :], piece, 0, 1)

    def pair_copy():
        return remote(
            proj.at[:, 1 - core], pair_in, send_sem.at[9], recv_all.at[2], at[1], q
        )

    def pair_total(chip):
        return proj[chip, core] + pair_in[chip]

    def across_chips():
        pair_copy().wait_recv()
        for k in reversed(range(2, sp_count, 2)):
            proj_out[k // 2] = pair_total(at[k] // 2).astype(proj_out.dtype)
            start(
                remote(
                    proj_out.at[k // 2],
                    proj_in.at[k // 2],
                    send_sem.at[10],
                    recv_all.at[3],
                    at[k],
                    q,
                )
            )
        grad_proj[...] = pair_total(me // 2)

    with jax.named_scope("project#m=0"):
        loads[12].wait()
        loads[13].wait()
        out_grad = project(0, 0)
        for j in range(1, halves):
            out_grad = out_grad + project(0, j)
    with jax.named_scope("grad_up"):
        input_grads(up_grad, grad_up)
    for j in range(halves):
        for m in range(1, tp_count):
            with jax.named_scope(f"gather#m={m}#j={j}"):
                piece = resid.at[:, half_columns(peer[m], j)]
                remote(piece, piece, send_sem.at[8], recv_ag.at[m - 1, j], me, q).wait_recv()
            with jax.named_scope(f"project#m={m}#j={j}"):
                out_grad = out_grad + project(m, j)
        if halves == 2:
            with jax.named_scope(f"pair#j={j}"):

                @pl.when(core != j)
                def _():
                    pair_copy().start()

                if j == 0:

                    @pl.when(core == j)
                    def _():
                        across_chips()

    if halves == 1:
        pair_copy().start()
    with jax.named_scope("query_states"):
        for h in range(heads):
            query = queries[key_part(h), :].astype(jnp.float32)
            for side in range(2):
                seen = exact_dot(query * reaches[reach_part(h, side), :], out_grad[value_part(h)], 1, 1)
                query_out[side, key_part(h), :] = seen.astype(query_out.dtype)
        for k in reversed(range(1, sp_count)):
            start(
                remote(
                    query_out.at[state_side(me, at[k], sp_count)],
                    query_all.at[me],
                    send_sem.at[11],
                    recv_all.at[4],
                    at[k],
                    q,
                )
            )
    with jax.named_scope("pair"):
        if halves == 1:
            across_chips()
        else:

            @pl.when(core == 1)
            def _():
                across_chips()

    with jax.named_scope("retention"):
        for h in range(heads):
            query = queries[key_part(h), :].astype(jnp.float32)
            key = keys[key_part(h), :].astype(jnp.float32)
            value = values[value_part(h), :].astype(jnp.float32)
            grad = out_grad[value_part(h)]
            score_grad = mixing[h] * exact_dot(grad, value, 0, 0)
            to_end = score_scale * reaches[reach_part(h, 0), :]
            from_start = score_scale * reaches[reach_part(h, 1), :]
            out_reach = jnp.concatenate([grad * from_start, grad * to_end], axis=0)
            grad_queries[key_part(h), :] = exact_dot(key, score_grad, 1, 1) + exact_dot(
                key_carried[h], out_reach, 1, 0
            )
            grad_keys[key_part(h), :] = exact_dot(query, score_grad, 1, 0)
            grad_values[value_part(h), :] = exact_dot(grad, scores[h], 1, 0)
    with jax.named_scope("query_wait"):
        piece = query_all.at[pl.ds(0, sp_count - 1)]
        remote(piece, piece, send_sem.at[11], recv_all.at[4], me, q).wait_recv()
    with jax.named_scope("finish"):
        for h in range(heads):
            key = keys[key_part(h), :].astype(jnp.float32)
            value = values[value_part(h), :].astype(jnp.float32)
            to_end = score_scale * reaches[reach_part(h, 0), :]
            from_start = score_scale * reaches[reach_part(h, 1), :]
            carried = []
            for decay in decays(h):
                total = jnp.zeros((key_size, value_size), jnp.float32)
                for b in range(sp_count):
                    total = total + decay[b] * query_all[b, key_part(h), :].astype(jnp.float32)
                carried.append(total)
            value_reach = jnp.concatenate([value * from_start, value * to_end], axis=0)
            key_reach = jnp.concatenate([key * from_start, key * to_end], axis=0)
            grad_keys[key_part(h), :] = grad_keys[key_part(h), :] + exact_dot(
                jnp.concatenate(carried, axis=1), value_reach, 1, 0
            )
            grad_values[value_part(h), :] = grad_values[value_part(h), :] + exact_dot(
                jnp.concatenate(carried, axis=0), key_reach, 0, 0
            )
    with jax.named_scope("proj_wait"):
        piece = proj_in.at[pl.ds(1, sp_count // 2 - 1)]
        remote(piece, piece, send_sem.at[10], recv_all.at[3], me, q).wait_recv()
        proj_total = grad_proj[...]
        for i in range(1, sp_count // 2):
            proj_total = proj_total + proj_in[i].astype(jnp.float32)
        grad_proj[...] = proj_total
    with jax.named_scope("sent"):
        others = pl.ds(0, sp_count - 2)
        crossing = 2 if square else tp_count - 1
        sent = [
            rows.at[:, others, :, pl.ds(0, width)],
            pair_src,
            rows.at[:, others, :, pl.ds(0, crossing * width)],
            rows.at[:, pl.ds(0, sp_count - 2 - len(direct)), :, pl.ds(0, width)] if square else None,
            state_all.at[pl.ds(0, sp_count - 1)],
            part.at[pl.ds(0, 2)] if square else part,
            part.at[2] if square else None,
            outgoing.at[pl.ds(0, sp_count - 1)],
            resid.at[:, pl.ds(0, (tp_count - 1) * width)],
            pair_in,
            proj_out.at[pl.ds(0, sp_count // 2 - 1)],
            query_all.at[pl.ds(0, sp_count - 1)],
            rows.at[:, pl.ds(0, len(direct)), :, pl.ds(0, width)] if square else None,
        ]
        for i, piece in enumerate(sent):
            if piece is not None:
                remote(piece, piece, send_sem.at[i], recv_all.at[0], me, q).wait_send()


def store_kernel(*refs):
    count = (len(refs) - 1) // 2
    copies = [
        pltpu.make_async_copy(refs[i], refs[count + i], refs[-1].at[i]) for i in range(count)
    ]
    for copy in copies:
        copy.start()
    for copy in copies:
        copy.wait()


def store(arrays):
    return pl.pallas_call(
        store_kernel,
        out_shape=tuple(jax.ShapeDtypeStruct(a.shape, a.dtype) for a in arrays),
        in_specs=[VMEM] * len(arrays),
        out_specs=(ANY,) * len(arrays),
        scratch_shapes=[pltpu.SemaphoreType.DMA((len(arrays),))],
        compiler_params=pltpu.CompilerParams(vmem_limit_bytes=16 * 1024 * 1024),
    )(*arrays)


def experts(
    ids, group, weight, rates, queries, keys, values, mixer, cot, inp, gate, up, down, proj, capacity, sp_count, tp_count
):
    tokens, model_width = cot.shape
    width = model_width // tp_count
    hidden_width = gate.shape[2]
    heads, length = rates.shape
    state_rows = keys.shape[0] + 8 * heads
    key_size = keys.shape[0] // heads
    value_size = values.shape[0] // heads
    head_columns = mixer.shape[1]
    proj_rows = model_width // sp_count
    block_rows = -(-capacity // 16) * 16
    all_rows = sp_count * block_rows
    chips = sp_count // 2
    quarter = sp_count // 4
    pairs = [0, 1] + list(range(sp_count // 2 - 1, 1, -1))
    order = [k for pair in pairs for k in (2 * pair, 2 * pair + 1)]
    groups = [(i * quarter, (i + 1) * quarter) for i in range(4)]
    crossing = 2 if tp_count == 4 else tp_count - 1
    kind = cot.dtype
    full = jnp.float32
    dma = pltpu.SemaphoreType.DMA
    vmem = pltpu.VMEM
    return pl.pallas_call(
        functools.partial(experts_kernel, sp_count, tp_count, order, groups),
        out_shape=(
            vmem((model_width, hidden_width), kind),
            vmem((model_width, hidden_width), kind),
            vmem((hidden_width, model_width), kind),
            vmem((proj_rows, head_columns), full),
            vmem(queries.shape, full),
            vmem(keys.shape, full),
            vmem(values.shape, full),
        ),
        in_specs=[ANY] * 14,
        out_specs=(VMEM,) * 7,
        scratch_shapes=[
            vmem(ids.shape, ids.dtype),
            vmem(group.shape, group.dtype),
            vmem(weight.shape, weight.dtype),
            vmem(rates.shape, rates.dtype),
            vmem(queries.shape, queries.dtype),
            vmem(keys.shape, keys.dtype),
            vmem(values.shape, values.dtype),
            vmem(mixer.shape, mixer.dtype),
            vmem((tokens, model_width), kind),
            vmem((tokens, model_width), kind),
            vmem((model_width, hidden_width), kind),
            vmem((model_width, hidden_width), kind),
            vmem((hidden_width, model_width), kind),
            vmem(proj.shape, kind),
            vmem((all_rows, ids.shape[0] * tokens), jnp.bfloat16),
            vmem((all_rows, tokens), jnp.bfloat16),
            vmem((ids.shape[0] * tokens, model_width), kind),
            vmem((sp_count, 2, block_rows, width), kind),
            vmem((quarter, 2, block_rows, width), kind),
            vmem((2, block_rows, model_width), kind),
            vmem((2, sp_count, block_rows, model_width), kind),
            vmem((2, state_rows, value_size), full),
            vmem((sp_count, state_rows, value_size), full),
            vmem((tokens, model_width), kind),
            vmem((heads, length, length), full),
            vmem((heads, length, length), full),
            vmem((8 * heads, length), full),
            vmem((heads, key_size, 2 * value_size), full),
            vmem((chips, 2, proj_rows, head_columns), full),
            vmem((chips, proj_rows, head_columns), full),
            vmem((chips, proj_rows, head_columns), kind),
            vmem((chips, proj_rows, head_columns), kind),
            vmem((2, keys.shape[0], value_size), kind),
            vmem((sp_count, keys.shape[0], value_size), kind),
            vmem((all_rows, hidden_width), kind),
            vmem((all_rows, hidden_width), kind),
            vmem((all_rows, hidden_width), kind),
            vmem((tp_count - 1, sp_count, block_rows, width), kind),
            vmem((sp_count, block_rows, width), full),
            vmem((sp_count, block_rows, width), full),
            vmem((tp_count - 1, sp_count, block_rows, width), kind),
            vmem((sp_count, block_rows, width), kind),
            vmem((sp_count, block_rows, width), kind),
            dma((14,)),
            dma((13,)),
            dma((sp_count,)),
            dma((sp_count - 2, crossing)),
            dma((2, sp_count - 2)),
            dma((len(groups), crossing)),
            dma((len(groups), 2)),
            dma((tp_count - 1, 2)),
            dma((5,)),
        ],
        compiler_params=pltpu.CompilerParams(
            collective_id=0, has_side_effects=True, vmem_limit_bytes=48 * 1024 * 1024
        ),
    )(ids, group, weight, rates, queries, keys, values, mixer, cot, inp, gate, up, down, proj)


def on_device(
    cotangent,
    moe_input,
    expert_ids,
    group_weight,
    expert_weight,
    mixer_out,
    queries,
    key_vectors,
    value_vectors,
    decay_rates,
    proj_weight,
    gate_weight,
    up_weight,
    down_weight,
):
    sp_count = lax.axis_size("sp")
    tp_count = lax.axis_size("tp")
    experts_all = gate_weight.shape[0] * sp_count
    rows_here = cotangent.shape[0]
    top_count = expert_ids.shape[1]
    capacity = 3 * top_count * rows_here // (2 * experts_all)
    results = experts(
        expert_ids.T,
        group_weight[None, :],
        expert_weight.T,
        decay_rates,
        queries,
        key_vectors,
        value_vectors,
        mixer_out,
        cotangent,
        moe_input,
        gate_weight,
        up_weight,
        down_weight,
        proj_weight,
        capacity,
        sp_count,
        tp_count,
    )
    grad_gate, grad_up, grad_down, grad_proj, grad_queries, grad_keys, grad_values = store(results)
    return (
        grad_gate[None],
        grad_up[None],
        grad_down[None],
        grad_proj,
        grad_queries,
        grad_keys,
        grad_values,
    )


def solution(mesh):
    return jax.shard_map(
        on_device,
        mesh=mesh,
        in_specs=(
            P("sp", None),
            P("sp", None),
            P("sp", None),
            P("sp"),
            P("sp", None),
            P("sp", "tp"),
            P("tp", "sp"),
            P("tp", "sp"),
            P("tp", "sp"),
            P("tp", "sp"),
            P(None, "tp"),
            P("sp", None, "tp"),
            P("sp", None, "tp"),
            P("sp", "tp", None),
        ),
        out_specs=(
            P("sp", None, "tp"),
            P("sp", None, "tp"),
            P("sp", "tp", None),
            P("sp", "tp"),
            P("tp", "sp"),
            P("tp", "sp"),
            P("tp", "sp"),
        ),
        check_vma=False,
    )
```
